128 devices in a mesh: sp: 64 (over z, y, x), tp: 2 (over core).
Axes of the slice: x: 4, y: 4, z: 4, core: 2. Of those that a mesh axis runs over, the one named last changes fastest.
Arguments:
- stream: bfloat16 [16384, 2048], P(('sp', 'tp')), may hold values from -6 to 6
- head_input_signal: bfloat16 [16384, 2048], P('sp', 'tp'), may hold values from -6 to 6
- write_input_vectors: bfloat16 [16384, 512], P('sp', 'tp'), may hold values from -6 to 6
- read_input_vectors: bfloat16 [16384, 512], P('sp', 'tp'), may hold values from -6 to 6
- output_gate_input: bfloat16 [16384, 2048], P('sp', 'tp'), may hold values from -6 to 6
- step_size_input: bfloat16 [16384, 32], P('sp', 'tp'), may hold values from -5 to 5.5
- position_log_decay: float32 [16384, 32], P('sp', 'tp'), may hold values from -0.7 to 0
- signal_filter_taps: bfloat16 [4, 2048], P(None, 'tp'), may hold values from -3 to 3
- write_filter_taps: bfloat16 [4, 512], P(None, 'tp'), may hold values from -3 to 3
- read_filter_taps: bfloat16 [4, 512], P(None, 'tp'), may hold values from -3 to 3
- step_size_bias: float32 [32], P('tp'), may hold values from -1 to 1
- head_decay_rate: float32 [32], P('tp'), may hold values from 6.1035156e-07 to 0.03
- head_direct_term: float32 [32], P('tp'), may hold values from 0.5 to 2
- grouped_norm_gain: float32 [2048], P('tp'), may hold values from 0.1 to 1.9
- mixer_output_weight: bfloat16 [2048, 2048], P('tp'), may hold values from -0.125 to 0.125
- expert_norm_gain: float32 [2048], replicated, may hold values from 0.1 to 1.9
- chosen_expert_index: int32 [16384, 4], P(('sp', 'tp')), may hold values from 0 to 127, all different within a row; in each aligned block of 128 rows (0 to 127, 128 to 255, ...) at most 6 rows name the same one
- chosen_expert_weight: float32 [16384, 4], P(('sp', 'tp')), may hold values from 0.1 to 1
- routed_gate_weight: bfloat16 [128, 2048, 512], P(('sp', 'tp')), may hold values from -0.125 to 0.125
- routed_up_weight: bfloat16 [128, 2048, 512], P(('sp', 'tp')), may hold values from -0.125 to 0.125
- routed_down_weight: bfloat16 [128, 512, 2048], P(('sp', 'tp')), may hold values from -0.25 to 0.25
- common_gate_weight: bfloat16 [2048, 512], replicated, may hold values from -0.125 to 0.125
- common_up_weight: bfloat16 [2048, 512], replicated, may hold values from -0.125 to 0.125
- common_down_weight: bfloat16 [512, 2048], replicated, may hold values from -0.25 to 0.25
Outputs:
- layer_out: bfloat16 [16384, 2048], P(('sp', 'tp'))
The draws below stay inside these ranges and needn't reach their ends.
Inputs may be any that keep to these rules, and one draw needn't show every extreme that they name: `chosen_expert_index`: each row names 4 different experts. Among the 128 rows of one device (aligned blocks of 128 rows) no expert is named more than 6 times; in some block one expert is named exactly 6 times.
All inputs are finite; a program needn't handle non-finite values.
Results may differ from the reference program's by a relative error of at most 0.015.
Values may be sent and summed in bfloat16 or wider, within the bound.
No kernel may reach another device: no remote copies, remote signals or barrier semaphores. Data moves between devices by JAX's collectives and lax.ppermute only.
A program may use at most 128 MiB of HBM per device.

```python
import math
import jax
import jax.numpy as jnp
import numpy as np
from jax import lax

D = 2048
HEADS = 32
HEAD_DIM = 64
GROUPS = 4
STATE = 128
CONV_K = 4
BLK = 128
EFF = 512
SFF = 512
TOP = 4
TOK_DEV = 256
SSM_WIDTH = 2048
TOKENS = 16384
ROWS = 128
EXPERTS = 128
CAP = 6
N_SP = 64
N_TP = 2


def draw_step_size_input(key, part):
    first_key, second_key = jax.random.split(jax.random.fold_in(key, 11))
    base = jnp.clip(jax.random.normal(first_key, (TOKENS, HEADS), jnp.float32), -4.0, 4.0)
    shifts = jax.random.uniform(second_key, (TOKENS // TOK_DEV, 1, 1), jnp.float32, -1.0, 1.5)
    shifts = jnp.broadcast_to(shifts, (TOKENS // TOK_DEV, TOK_DEV, HEADS)).reshape(TOKENS, HEADS)
    return (base + shifts).astype(jnp.bfloat16)


def draw_position_log_decay(key, part):
    first_key, second_key = jax.random.split(jax.random.fold_in(key, 23))
    spots = jax.random.randint(first_key, (8,), 0, TOKENS)
    struck = jnp.any(jnp.arange(TOKENS)[:, None] == spots[None, :], axis=1)
    values = jax.random.uniform(second_key, (TOKENS, HEADS), jnp.float32, -0.69, -0.22)
    return jnp.where(struck[:, None], values, 0.0).astype(jnp.float32)


def draw_head_decay_rate(key, part):
    lowest = math.log(0.01 / TOKENS)
    highest = math.log(0.03)
    logs = jax.random.uniform(jax.random.fold_in(key, 37), (HEADS,), jnp.float32, lowest, highest)
    return jnp.exp(logs).astype(jnp.float32)


def block_scale(key, dims, shards, smallest, top_value):
    factor_of, own = 1.0, jax.random.fold_in(key, 6)
    for axis_at, blocks in shards:
        heights = jnp.exp(jax.random.uniform(jax.random.fold_in(own, axis_at), (blocks,), jnp.float32, smallest / len(shards), top_value / len(shards)))
        factor_of = factor_of * jnp.repeat(heights, dims[axis_at] // blocks).reshape([-1 if axis == axis_at else 1 for axis in range(len(dims))])
    return factor_of


def routed_block(stream_key, own, number, rows, number_of, top, bound, lean):
    order = jax.random.permutation(stream_key, number_of)
    packed, ordinary = shares(number_of, rows * top, bound, lean, True), shares(number_of, rows * top, bound, lean, False)
    places = jnp.arange(number_of)

    def named(tallies, turn):
        used = int((tallies > 0).sum())
        fixed = max(1, used // 4)
        shifted = fixed + (places - fixed + turn * (used - fixed)) % max(1, number_of - fixed)
        return jnp.zeros((number_of,), jnp.int32).at[order[jnp.where(places < fixed, places, shifted)]].set(jnp.asarray(tallies, jnp.int32))

    tallies = jnp.where(number % 4 == 0, named(packed, number // 4), named(ordinary, number - number // 4 - 1))
    mixed = jax.random.permutation(jax.random.fold_in(own, 3), number_of)
    giver, sink = mixed[0:number_of // 2 * 2:2], mixed[1:number_of // 2 * 2:2]
    room = jnp.minimum(tallies[giver] - 1, bound - tallies[sink]) // 2
    room = jnp.where((giver == order[0]) | (sink == order[0]) | (tallies[sink] == 0), 0, jnp.maximum(room, 0))
    shifted = jax.random.randint(jax.random.fold_in(own, 4), (number_of // 2,), 0, 1 << 20) % (room + 1)
    tallies = tallies.at[giver].add(-shifted).at[sink].add(shifted)
    members = jnp.searchsorted(jnp.cumsum(tallies), jnp.arange(rows * top), side="right").astype(jnp.int32)
    table = members.reshape(top, rows).T
    table = table[jax.random.permutation(jax.random.fold_in(own, 1), rows)]
    turn = jax.random.randint(jax.random.fold_in(own, 2), (rows, 1), 0, top)
    return jnp.take_along_axis(table, (jnp.arange(top)[None, :] + turn) % top, axis=1)


def shares(amount, total, limit, slope, full):
    loads = [(1 << 20) // math.isqrt(standing ** slope) + 1 for standing in range(1, amount + 1)]
    largest = limit if full else min(limit, max(-(-total // amount), total * loads[0] // sum(loads)))
    least = 1 if total - largest >= amount - 1 else 0
    given, rest = [largest] + [least] * (amount - 1), total - largest - least * (amount - 1)
    while rest > 0:
        free = [i for i in range(1, amount) if given[i] < largest] or [i for i in range(1, amount) if given[i] < limit]
        pool, budget = sum([loads[i] for i in free]), rest
        for i in free:
            more = min(limit - given[i], max(1, budget * loads[i] // pool), rest)
            given[i] = given[i] + more
            rest = rest - more
    return np.array(given)


def scatter_about(stream_key, extent, deviation, reach, cuts=(), kind=jnp.bfloat16):
    loudness = block_scale(stream_key, extent, cuts, -0.22, 0.18) if cuts else 1.0
    drawn = jax.random.normal(stream_key, extent, jnp.float32) * deviation * loudness
    return jnp.minimum(jnp.maximum(drawn, -reach), reach).astype(kind)


def setup_inputs(seed: int = 0) -> dict:
    arg_keys = jax.random.split(jax.random.key(seed), 25)
    stream = scatter_about(arg_keys[0], (TOKENS, D), 1.0, 6.0, ((0, 128),))
    head_input_signal = scatter_about(arg_keys[1], (TOKENS, SSM_WIDTH), 1.0, 6.0, ((0, 64), (1, 2)))
    write_input_vectors = scatter_about(arg_keys[2], (TOKENS, GROUPS * STATE), 1.0, 6.0, ((0, 64), (1, 2)))
    read_input_vectors = scatter_about(arg_keys[3], (TOKENS, GROUPS * STATE), 1.0, 6.0, ((0, 64), (1, 2)))
    output_gate_input = scatter_about(arg_keys[4], (TOKENS, SSM_WIDTH), 1.0, 6.0, ((0, 64), (1, 2)))
    step_size_input = draw_step_size_input(jax.random.fold_in(arg_keys[24], 71), 0)
    position_log_decay = draw_position_log_decay(jax.random.fold_in(arg_keys[24], 71), 0)
    signal_filter_taps = scatter_about(arg_keys[7], (CONV_K, SSM_WIDTH), CONV_K ** -0.5, 3.0, ((1, 2),))
    write_filter_taps = scatter_about(arg_keys[8], (CONV_K, GROUPS * STATE), CONV_K ** -0.5, 3.0, ((1, 2),))
    read_filter_taps = scatter_about(arg_keys[9], (CONV_K, GROUPS * STATE), CONV_K ** -0.5, 3.0, ((1, 2),))
    step_size_bias = jnp.clip(jax.random.uniform(arg_keys[10], (HEADS,), jnp.float32, -1.0, 1.0) * block_scale(arg_keys[10], (HEADS,), ((0, 2),), -0.4, 0.0), -1.0, 1.0)
    head_decay_rate = draw_head_decay_rate(jax.random.fold_in(arg_keys[24], 71), 0)
    head_direct_term = jnp.clip(0.5 + 1.5 * jax.random.uniform(arg_keys[12], (HEADS,), jnp.float32) ** block_scale(arg_keys[12], (HEADS,), ((0, 2),), -0.2, 0.2), 0.5, 2.0)
    grouped_norm_gain = jnp.clip(1.0 + 0.18 * jax.random.normal(arg_keys[13], (SSM_WIDTH,), jnp.float32), 0.1, 1.9)
    mixer_output_weight = scatter_about(arg_keys[14], (SSM_WIDTH, D), SSM_WIDTH ** -0.5, 0.125, ((0, 2),))
    expert_norm_gain = jnp.clip(1.0 + 0.18 * jax.random.normal(arg_keys[15], (D,), jnp.float32), 0.1, 1.9)
    chosen_expert_index_keys = jax.random.split(jax.random.fold_in(arg_keys[16], 1), TOKENS // ROWS)
    chosen_expert_index_turns = jax.random.permutation(jax.random.fold_in(arg_keys[16], 3), TOKENS // ROWS)
    chosen_expert_index = jax.vmap(lambda own, number: routed_block(jax.random.fold_in(arg_keys[16], 2), own, number, ROWS, EXPERTS, TOP, CAP, 1))(chosen_expert_index_keys, chosen_expert_index_turns).reshape((TOKENS, TOP))
    chosen_expert_weight = jnp.clip(0.1 + 0.9 * jax.random.uniform(arg_keys[17], (TOKENS, TOP), jnp.float32) ** block_scale(arg_keys[17], (TOKENS, TOP), ((0, 128),), -0.2, 0.2), 0.1, 1.0)
    routed_gate_weight = scatter_about(arg_keys[18], (EXPERTS, D, EFF), D ** -0.5, 0.125, ((0, 128),))
    routed_up_weight = scatter_about(arg_keys[19], (EXPERTS, D, EFF), D ** -0.5, 0.125, ((0, 128),))
    routed_down_weight = scatter_about(arg_keys[20], (EXPERTS, EFF, D), EFF ** -0.5, 0.25, ((0, 128),))
    common_gate_weight = scatter_about(arg_keys[21], (D, SFF), D ** -0.5, 0.125)
    common_up_weight = scatter_about(arg_keys[22], (D, SFF), D ** -0.5, 0.125)
    common_down_weight = scatter_about(arg_keys[23], (SFF, D), SFF ** -0.5, 0.25)
    return {"stream": stream, "head_input_signal": head_input_signal, "write_input_vectors": write_input_vectors, "read_input_vectors": read_input_vectors, "output_gate_input": output_gate_input, "step_size_input": step_size_input, "position_log_decay": position_log_decay, "signal_filter_taps": signal_filter_taps, "write_filter_taps": write_filter_taps, "read_filter_taps": read_filter_taps, "step_size_bias": step_size_bias, "head_decay_rate": head_decay_rate, "head_direct_term": head_direct_term, "grouped_norm_gain": grouped_norm_gain, "mixer_output_weight": mixer_output_weight, "expert_norm_gain": expert_norm_gain, "chosen_expert_index": chosen_expert_index, "chosen_expert_weight": chosen_expert_weight, "routed_gate_weight": routed_gate_weight, "routed_up_weight": routed_up_weight, "routed_down_weight": routed_down_weight, "common_gate_weight": common_gate_weight, "common_up_weight": common_up_weight, "common_down_weight": common_down_weight}


precise = lax.Precision.HIGHEST

def causal_conv(previous, current, weight):
    stacked = jnp.concatenate([previous, current], axis=0).astype(jnp.float32)
    weight = weight.astype(jnp.float32)
    kernel_len = weight.shape[0]
    length = current.shape[0]
    summed_taps = weight[0] * stacked[0:length]
    for offset in range(1, kernel_len):
        summed_taps = summed_taps + weight[offset] * stacked[offset:offset + length]
    return jax.nn.silu(summed_taps)

def reference(stream, head_input_signal, write_input_vectors, read_input_vectors, output_gate_input, step_size_input, position_log_decay, signal_filter_taps, write_filter_taps, read_filter_taps, step_size_bias, head_decay_rate, head_direct_term, grouped_norm_gain, mixer_output_weight, expert_norm_gain, chosen_expert_index, chosen_expert_weight, routed_gate_weight, routed_up_weight, routed_down_weight, common_gate_weight, common_up_weight, common_down_weight):
    margin = CONV_K - 1
    signal = causal_conv(jnp.zeros((margin, SSM_WIDTH), jnp.bfloat16), head_input_signal, signal_filter_taps)
    write_vec = causal_conv(jnp.zeros((margin, GROUPS * STATE), jnp.bfloat16), write_input_vectors, write_filter_taps)
    read_vec = causal_conv(jnp.zeros((margin, GROUPS * STATE), jnp.bfloat16), read_input_vectors, read_filter_taps)
    time_position = jax.nn.softplus(step_size_input.astype(jnp.float32) + step_size_bias)
    decay_logarithm = position_log_decay - head_decay_rate * time_position
    per_group = HEADS // GROUPS
    blocks = TOKENS // BLK
    signal_heads = signal.reshape(TOKENS, GROUPS, per_group, HEAD_DIM)
    scaled_in = signal_heads * time_position.reshape(TOKENS, GROUPS, per_group)[..., None]
    causal = jnp.arange(BLK)[:, None] >= jnp.arange(BLK)[None, :]
    skip_heads = head_direct_term.reshape(GROUPS, per_group)[:, :, None]

    def advance(carry_state, inputs):
        scaled_blk, write_blk, read_blk, decay_blk, signal_blk = inputs
        within_cum = jnp.cumsum(decay_blk, axis=0)
        cum_heads = jnp.transpose(within_cum, (1, 2, 0))
        decay_matrix = jnp.exp(jnp.where(causal, cum_heads[..., :, None] - cum_heads[..., None, :], -jnp.inf))
        intersection = jnp.einsum('tgn,sgn->gts', read_blk, write_blk, precision=precise)
        intra = jnp.einsum('gts,gets,sgep->tgep', intersection, decay_matrix, scaled_blk, precision=precise)
        carried = jnp.einsum('tgn,gepn,tge->tgep', read_blk, carry_state, jnp.exp(within_cum), precision=precise)
        tail_decay = jnp.exp(within_cum[-1][None] - within_cum)
        fresh = jnp.einsum('sgn,sge,sgep->gepn', write_blk, tail_decay, scaled_blk, precision=precise)
        next_state = carry_state * jnp.exp(within_cum[-1])[..., None, None] + fresh
        return (next_state, intra + carried + skip_heads * signal_blk)
    sequence = (scaled_in.reshape(blocks, BLK, GROUPS, per_group, HEAD_DIM), write_vec.reshape(blocks, BLK, GROUPS, STATE), read_vec.reshape(blocks, BLK, GROUPS, STATE), decay_logarithm.reshape(blocks, BLK, GROUPS, per_group), signal_heads.reshape(blocks, BLK, GROUPS, per_group, HEAD_DIM))
    initial = jnp.zeros((GROUPS, per_group, HEAD_DIM, STATE), jnp.float32)
    ssd_out = lax.scan(advance, initial, sequence)[1]
    gated = ssd_out.reshape(TOKENS, GROUPS, per_group * HEAD_DIM) * jax.nn.silu(output_gate_input.astype(jnp.float32)).reshape(TOKENS, GROUPS, per_group * HEAD_DIM)
    norm_scale = lax.rsqrt(lax.optimization_barrier(jnp.mean(gated * gated, axis=-1, keepdims=True)) + 1e-06)
    mixer_out = ((gated * norm_scale).reshape(TOKENS, SSM_WIDTH) * grouped_norm_gain).astype(jnp.bfloat16)
    residual = (stream.astype(jnp.float32) + jnp.dot(mixer_out, mixer_output_weight, preferred_element_type=jnp.float32)).astype(jnp.bfloat16)
    widened = residual.astype(jnp.float32)
    normed = (widened * lax.rsqrt(lax.optimization_barrier(jnp.mean(widened * widened, axis=-1, keepdims=True)) + 1e-06) * expert_norm_gain).astype(jnp.bfloat16)
    shared_hidden = (jax.nn.silu(jnp.dot(normed, common_gate_weight, preferred_element_type=jnp.float32)) * jnp.dot(normed, common_up_weight, preferred_element_type=jnp.float32)).astype(jnp.bfloat16)
    shared = jnp.dot(shared_hidden, common_down_weight, preferred_element_type=jnp.float32)
    row_total = TOKENS * TOP
    chosen = chosen_expert_index.reshape(-1).astype(jnp.int32)
    one_hot = (chosen[:, None] == jnp.arange(EXPERTS, dtype=jnp.int32)[None, :]).astype(jnp.int32)
    slot_index = lax.optimization_barrier(jnp.sum((jnp.cumsum(one_hot, axis=0) - one_hot) * one_hot, axis=1)).astype(jnp.int32)
    slot_limit = N_SP * N_TP * CAP
    source_row = (jnp.arange(row_total, dtype=jnp.int32) // TOP).astype(jnp.int32)
    slot_table = jnp.full((EXPERTS, slot_limit), TOKENS, jnp.int32).at[chosen, slot_index].set(source_row)
    weight_table = jnp.zeros((EXPERTS, slot_limit), jnp.float32).at[chosen, slot_index].set(chosen_expert_weight.reshape(-1))
    padded = jnp.concatenate([normed, jnp.zeros((1, D), normed.dtype)], axis=0)

    def serve_expert(summed, inputs):
        gate_w, up_w, down_w, indices, weights = inputs
        picked = padded[indices]
        hidden = (jax.nn.silu(jnp.dot(picked, gate_w, preferred_element_type=jnp.float32)) * jnp.dot(picked, up_w, preferred_element_type=jnp.float32)).astype(jnp.bfloat16)
        result = jnp.dot(hidden, down_w, preferred_element_type=jnp.float32).astype(jnp.bfloat16)
        return (summed.at[indices].add(weights[:, None] * result.astype(jnp.float32), mode='drop'), None)
    routed = lax.scan(serve_expert, jnp.zeros((TOKENS, D), jnp.float32), (routed_gate_weight, routed_up_weight, routed_down_weight, slot_table, weight_table))[0]
    return (widened + shared + routed).astype(jnp.bfloat16)
```

```python
import jax
import jax.numpy as jnp
from jax import lax
from jax.experimental import pallas as pl
from jax.experimental.pallas import tpu as pltpu
from jax.sharding import Mesh
from jax.sharding import PartitionSpec as P

HEAD_DIM = 64
STATE = 128
BLK = 128
LANES = 128
SLOTS = 6
WIDE = 8
SP = ("sp_0", "sp_1", "sp_2")
PLANE = ("sp_1", "sp_2")
SP_TP = ("sp_0", "sp_1", "sp_2", "tp")
F32 = jnp.float32
BF16 = jnp.bfloat16


def mm(a, b, dims=((1,), (0,)), precision=None):
    return lax.dot_general(a, b, (dims, ((), ())), precision=precision, preferred_element_type=F32)


def iota(shape, dim):
    return lax.broadcasted_iota(jnp.int32, shape, dim)


def head_lanes(width):
    return jnp.where(iota((LANES, width), 1) // HEAD_DIM == iota((LANES, width), 0), 1.0, 0.0).astype(BF16)


def spread(values, lanes):
    high = values.astype(BF16)
    low = (values - high.astype(F32)).astype(BF16)
    return mm(high, lanes) + mm(low, lanes)


def silu(v):
    return v * (1.0 / (1.0 + jnp.exp(-v)))


def whole(shape):
    return pl.BlockSpec(shape, lambda *_: (0,) * len(shape))


def front_kernel(x_ref, b_ref, c_ref, rim_ref, dt_ref, pld_ref, tx_ref, tb_ref, tc_ref, bias_ref, rate_ref,
                 sig_ref, wv_ref, rv_ref, cum_ref, dtv_ref, s0_ref, send_ref, ext_ref):
    length, chans = x_ref.shape
    vecs = b_ref.shape[1]
    heads = dt_ref.shape[1]
    groups = vecs // STATE
    width = chans // groups
    sources = ((x_ref, tx_ref, 0, chans, sig_ref), (b_ref, tb_ref, chans, vecs, wv_ref), (c_ref, tc_ref, chans + vecs, vecs, rv_ref))
    for src, taps, start, size, dst in sources:
        ext_ref[0:8, start : start + size] = rim_ref[:, start : start + size].astype(F32)
        ext_ref[8 : 8 + length, start : start + size] = src[...].astype(F32)
        for at in range(0, size, 256):
            lanes = slice(start + at, start + at + 256)
            weight = taps[:, at : at + 256].astype(F32)
            total = weight[0:1] * ext_ref[5 : 5 + length, lanes]
            for k in range(1, 4):
                total = total + weight[k : k + 1] * ext_ref[5 + k : 5 + k + length, lanes]
            dst[:, at : at + 256] = silu(total).astype(dst.dtype)
    v = dt_ref[...].astype(F32) + bias_ref[...]
    step = jnp.maximum(v, 0.0) + jnp.log(1.0 + jnp.exp(-jnp.abs(v)))
    logs = pld_ref[...] - rate_ref[...] * step
    dtv_ref[...] = jnp.zeros_like(dtv_ref)
    cum_ref[...] = jnp.zeros_like(cum_ref)
    dtv_ref[:, 0:heads] = step
    cum_ref[:, 0:heads] = logs
    lower = jnp.where(iota((length, length), 0) >= iota((length, length), 1), 1.0, 0.0)
    cum = mm(lower, cum_ref[...], precision=lax.Precision.HIGHEST)
    cum_ref[...] = cum
    half_end, end = cum[BLK - 1 : BLK], cum[length - 1 : length]
    ends = jnp.where(iota((length, LANES), 0) < BLK, half_end, end)
    lanes = head_lanes(chans)
    scaled = (sig_ref[...] * spread(dtv_ref[...] * jnp.exp(ends - cum), lanes)).astype(BF16)
    passing = spread(jnp.broadcast_to(jnp.exp(end - half_end), (8, LANES)), lanes)[0:1]
    for g in range(groups):
        part = slice(g * width, (g + 1) * width)
        vec = slice(g * STATE, (g + 1) * STATE)
        first = mm(wv_ref[0:BLK, vec], scaled[0:BLK, part], ((0,), (0,)))
        second = mm(wv_ref[BLK:length, vec], scaled[BLK:length, part], ((0,), (0,)))
        s0_ref[:, part] = first
        send_ref[:, part] = (first * passing[:, part] + second).astype(BF16)
    high = end.astype(BF16).astype(F32)
    mid = (end - high).astype(BF16).astype(F32)
    low = (end - high - mid).astype(BF16).astype(F32)
    row = iota((STATE, LANES), 0) % 8
    send_ref[:, chans : chans + LANES] = jnp.where(
        row == 0, high, jnp.where(row == 1, mid, jnp.where(row == 2, low, 0.0))
    ).astype(BF16)


def plane_kernel(got_ref, pin_ref, pdec_ref, send_ref):
    count = got_ref.shape[0] // 8
    chans = got_ref.shape[1] - LANES
    logs = jnp.sum(got_ref[:, chans:].astype(F32).reshape(count, 8, LANES), axis=1)
    lanes = head_lanes(chans)
    decay = spread(jnp.exp(logs), lanes)
    state = jnp.zeros((8, chans), F32)
    sofar = jnp.zeros((1, LANES), F32)
    before = []
    for i in range(count):
        pin_ref[8 * i : 8 * i + 8, :] = state
        before.append(sofar)
        state = state * decay[i : i + 1] + got_ref[8 * i : 8 * i + 8, 0:chans].astype(F32)
        sofar = sofar + logs[i : i + 1]
    pdec_ref[...] = spread(jnp.exp(jnp.concatenate(before, axis=0)), lanes)
    send_ref[:, 0:chans] = state
    send_ref[:, chans:] = jnp.broadcast_to(sofar, (8, LANES))


def planes_kernel(pin_ref, pdec_ref, one_ref, two_ref, three_ref, out_ref):
    chans = pin_ref.shape[1]
    count = pin_ref.shape[0] // 8
    lanes = head_lanes(chans)
    near = spread(jnp.exp(one_ref[:, chans:]), lanes)
    far = spread(jnp.exp(two_ref[:, chans:]), lanes)
    state = one_ref[:, 0:chans] + near * (two_ref[:, 0:chans] + far * three_ref[:, 0:chans])
    for i in range(0, count, 2):
        pair = [pin_ref[8 * k : 8 * k + 8, :] + state * pdec_ref[k : k + 1, :] for k in (i, i + 1)]
        out_ref[8 * i : 8 * i + 16, :] = jnp.concatenate(pair, axis=0).astype(BF16)


def near_kernel(sig_ref, wv_ref, rv_ref, cum_ref, dtv_ref, s0_ref, direct_ref, y_ref, pad_ref):
    length, chans = sig_ref.shape
    heads = direct_ref.shape[1]
    groups = wv_ref.shape[1] // STATE
    width = chans // groups
    lanes = head_lanes(chans)
    cum = cum_ref[...]
    cum_rows = cum.T
    pad_ref[...] = jnp.zeros_like(pad_ref)
    pad_ref[:, 0:heads] = jnp.broadcast_to(direct_ref[...], (8, heads))
    direct = spread(pad_ref[...], lanes)[0:1]
    scaled = (sig_ref[...] * spread(dtv_ref[...], lanes)).astype(BF16)
    causal = iota((BLK, BLK), 0) >= iota((BLK, BLK), 1)
    left = iota((BLK, LANES), 1) < HEAD_DIM
    into = spread(jnp.exp(cum[BLK:length] - cum[BLK - 1 : BLK]), lanes)
    for b in range(length // BLK):
        rows = slice(b * BLK, (b + 1) * BLK)
        for g in range(groups):
            vec = slice(g * STATE, (g + 1) * STATE)
            part = slice(g * width, (g + 1) * width)
            products = mm(rv_ref[rows, vec], wv_ref[rows, vec], ((1,), (1,)))
            if b == 1:
                carried = mm(rv_ref[rows, vec], s0_ref[:, part].astype(BF16)) * into[:, part]
            for j in range(width // LANES):
                at = g * width + j * LANES
                mats = []
                for h in (at // HEAD_DIM, at // HEAD_DIM + 1):
                    gap = cum[rows, h : h + 1] - cum_rows[h : h + 1, rows]
                    mats.append((products * jnp.exp(jnp.where(causal, gap, -1e30))).astype(BF16))
                pair = scaled[rows, at : at + LANES]
                zero = jnp.zeros_like(pair)
                stacked = jnp.concatenate([jnp.where(left, pair, zero), jnp.where(left, zero, pair)], axis=0)
                out = mm(jnp.concatenate(mats, axis=1), stacked)
                out = out + direct[:, at : at + LANES] * sig_ref[rows, at : at + LANES]
                if b == 1:
                    out = out + carried[:, j * LANES : (j + 1) * LANES]
                y_ref[rows, at : at + LANES] = out


def project_kernel(half_ref, y_ref, state_ref, rv_ref, cum_ref, gate_ref, gain_ref, w_ref, own_ref, other_ref, mix_ref, res_ref):
    length, chans = y_ref.shape
    groups = rv_ref.shape[1] // STATE
    width = chans // groups
    rows = own_ref.shape[0]

    @pl.when(pl.program_id(0) == 0)
    def _():
        scale = spread(jnp.exp(cum_ref[...]), head_lanes(chans))
        for g in range(groups):
            part = slice(g * width, (g + 1) * width)
            far = mm(rv_ref[:, g * STATE : (g + 1) * STATE], state_ref[:, part])
            gated = (y_ref[:, part] + far * scale[:, part]) * silu(gate_ref[:, part].astype(F32))
            mean = jnp.sum(gated * gated, axis=1, keepdims=True) * (1.0 / width)
            mix_ref[:, part] = (gated * lax.rsqrt(mean + 1e-06) * gain_ref[:, part]).astype(BF16)

    res_ref[...] = mm(mix_ref[...], w_ref[...])
    half = half_ref[0]
    own_ref[...] = res_ref[pl.ds(pl.multiple_of(half * rows, rows), rows), :]
    other_ref[...] = res_ref[pl.ds(pl.multiple_of((1 - half) * rows, rows), rows), :].astype(BF16)


def slot_table(chosen, experts):
    count = chosen.shape[0]
    expert = iota((count, experts), 1)
    named = jnp.zeros((count, experts), F32)
    for k in range(chosen.shape[1]):
        named = named + jnp.where(chosen[:, k : k + 1] == expert, 1.0, 0.0)
    earlier = jnp.where(iota((count, count), 0) > iota((count, count), 1), 1.0, 0.0).astype(BF16)
    rank = mm(earlier, named.astype(BF16))
    return named * (rank + 1.0)


def expert_rows(experts):
    return jnp.where(iota((experts * WIDE, experts), 0) // WIDE == iota((experts * WIDE, experts), 1), 1.0, 0.0).astype(BF16)


def dispatch_kernel(own_ref, got_ref, stream_ref, gain_ref, chosen_ref, residual_ref, normed_ref, out_ref, both_ref):
    rows, dim = own_ref.shape
    third = out_ref.shape[1] // 3
    experts = out_ref.shape[0] // WIDE
    residual = (stream_ref[...].astype(F32) + own_ref[...] + got_ref[...].astype(F32)).astype(BF16)
    residual_ref[...] = residual
    wide = residual.astype(F32)
    mean = jnp.sum(wide * wide, axis=1, keepdims=True) * (1.0 / dim)
    normed_ref[...] = (wide * lax.rsqrt(mean + 1e-06) * gain_ref[...]).astype(BF16)
    table = slot_table(chosen_ref[...], experts)
    slots = mm(expert_rows(experts), table.astype(BF16), ((1,), (1,)))
    place = (iota(slots.shape, 0) % WIDE).astype(F32)
    main = jnp.where(slots == place + 1.0, 1.0, 0.0)
    for q in range(3):
        tail = jnp.where((place >= 6.0) & (slots == 3.0 * place + (q - 17.0)), 1.0, 0.0)
        both_ref[:, 0:rows] = main.astype(BF16)
        both_ref[:, rows:] = tail.astype(BF16)
        source = jnp.concatenate([normed_ref[:, q * third : (q + 1) * third], normed_ref[:, 3 * third :]], axis=0)
        out_ref[:, q * third : (q + 1) * third] = mm(both_ref[...], source).astype(BF16)


def shared_kernel(normed_ref, residual_ref, gate_ref, up_ref, down_ref, out_ref):
    @pl.when(pl.program_id(0) == 0)
    def _():
        out_ref[...] = residual_ref[...].astype(F32)

    normed = normed_ref[...]
    hidden = (silu(mm(normed, gate_ref[...])) * mm(normed, up_ref[...])).astype(BF16)
    out_ref[...] += mm(hidden, down_ref[...])


def expert_kernel(x_ref, gate_ref, up_ref, down_ref, out_ref, full_ref):
    rows, wide = x_ref.shape
    third = wide // 3
    row, col = iota((LANES, LANES), 0), iota((LANES, LANES), 1)
    same = row // WIDE == col // WIDE
    r, c = row % WIDE, col % WIDE
    unpack = [jnp.where(same & (c >= 6) & (r == 3 * (c - 6) + q), 1.0, 0.0).astype(BF16) for q in range(3)]
    pack = [jnp.where(same & (r >= 6) & (c == 3 * (r - 6) + q), 1.0, 0.0).astype(BF16) for q in range(3)]
    unpack, pack = jnp.concatenate(unpack, axis=1), jnp.concatenate(pack, axis=0)
    full_ref[:, 0:wide] = x_ref[...]
    for at in range(0, rows, LANES):
        pieces = [x_ref[at : at + LANES, q * third : (q + 1) * third] for q in range(3)]
        full_ref[at : at + LANES, wide:] = mm(unpack, jnp.concatenate(pieces, axis=0)).astype(BF16)
    full = full_ref[...]
    hidden = (silu(mm(full, gate_ref[...])) * mm(full, up_ref[...])).astype(BF16)
    tail = mm(hidden, down_ref[:, wide:]).astype(BF16)
    inside = iota((LANES, third), 0) % WIDE < SLOTS
    packed = [mm(pack, tail[at : at + LANES]) for at in range(0, rows, LANES)]
    for q in range(3):
        part = slice(q * third, (q + 1) * third)
        result = mm(hidden, down_ref[:, part])
        for k, at in enumerate(range(0, rows, LANES)):
            extra = packed[k][q * LANES : (q + 1) * LANES]
            out_ref[at : at + LANES, part] = jnp.where(inside, result[at : at + LANES], extra).astype(BF16)


def combine_kernel(got_ref, base_ref, chosen_ref, weight_ref, out_ref, mats_ref, tail_ref):
    rows, dim = base_ref.shape
    third = got_ref.shape[1]
    experts = got_ref.shape[0] // WIDE
    q = pl.program_id(0)

    @pl.when(q == 0)
    def _():
        chosen = chosen_ref[...]
        table = slot_table(chosen, experts)
        expert = iota((rows, experts), 1)
        weights = jnp.zeros((rows, experts), F32)
        for k in range(chosen.shape[1]):
            weights = weights + jnp.where(chosen[:, k : k + 1] == expert, weight_ref[:, k : k + 1], 0.0)
        lanes = expert_rows(experts)
        slots = mm(table.astype(BF16), lanes, ((1,), (1,)))
        spread_weights = mm(weights.astype(BF16), lanes, ((1,), (1,)))
        place = (iota(slots.shape, 1) % WIDE).astype(F32)
        mats_ref[0:rows, :] = jnp.where(slots == place + 1.0, spread_weights, 0.0).astype(BF16)
        for k in range(3):
            hit = (place >= 6.0) & (slots == 3.0 * place + (k - 17.0))
            mats_ref[rows * (k + 1) : rows * (k + 2), :] = jnp.where(hit, spread_weights, 0.0).astype(BF16)
        tail_ref[...] = base_ref[:, 3 * third :]

    got = got_ref[...]
    tail_ref[...] += mm(mats_ref[pl.ds(pl.multiple_of(rows * (q + 1), rows), rows), :], got)
    main = mm(mats_ref[0:rows, :], got)
    for k in range(3):
        @pl.when(q == k)
        def _():
            part = slice(k * third, (k + 1) * third)
            out_ref[:, part] = (base_ref[:, part] + main).astype(BF16)

    @pl.when(q == 2)
    def _():
        out_ref[:, 3 * third :] = tail_ref[...].astype(BF16)


def shape(dims, dtype=F32):
    return jax.ShapeDtypeStruct(dims, dtype)


def on_device(
    stream,
    head_input_signal,
    write_input_vectors,
    read_input_vectors,
    output_gate_input,
    step_size_input,
    position_log_decay,
    signal_filter_taps,
    write_filter_taps,
    read_filter_taps,
    step_size_bias,
    head_decay_rate,
    head_direct_term,
    grouped_norm_gain,
    mixer_output_weight,
    expert_norm_gain,
    chosen_expert_index,
    chosen_expert_weight,
    routed_gate_weight,
    routed_up_weight,
    routed_down_weight,
    common_gate_weight,
    common_up_weight,
    common_down_weight,
):
    length, chans = head_input_signal.shape
    vecs = write_input_vectors.shape[1]
    rows, dim = stream.shape
    hidden = common_gate_weight.shape[1]
    experts = lax.axis_size(SP_TP)
    wide = dim * SLOTS // WIDE

    rim = jnp.concatenate([head_input_signal[length - 8 :], write_input_vectors[length - 8 :], read_input_vectors[length - 8 :]], axis=1)
    devices = lax.axis_size(SP)
    rim = lax.ppermute(rim, SP, [(i, i + 1) for i in range(devices - 1)])
    sig, wv, rv, cum, dtv, s0, send = pl.pallas_call(
        front_kernel,
        out_shape=(
            shape((length, chans)), shape((length, vecs), BF16), shape((length, vecs), BF16), shape((length, LANES)),
            shape((length, LANES)), shape((STATE, chans)), shape((STATE, chans + LANES), BF16),
        ),
        scratch_shapes=[pltpu.VMEM((length + 8, chans + 2 * vecs), F32)],
        name="front",
    )(
        head_input_signal, write_input_vectors, read_input_vectors, rim, step_size_input, position_log_decay,
        signal_filter_taps, write_filter_taps, read_filter_taps, step_size_bias[None], head_decay_rate[None],
    )
    in_plane = lax.axis_size(PLANE)
    got = lax.all_to_all(send, PLANE, split_axis=0, concat_axis=0, tiled=True)
    near = pl.pallas_call(
        near_kernel,
        out_shape=shape((length, chans)),
        scratch_shapes=[pltpu.VMEM((8, LANES), F32)],
        cost_estimate=pl.CostEstimate(flops=400_000_000, transcendentals=1_000_000, bytes_accessed=4_000_000),
        name="near",
    )(sig, wv, rv, cum, dtv, s0, head_direct_term[None])
    pin, pdec, total = pl.pallas_call(
        plane_kernel,
        out_shape=(shape((STATE, chans)), shape((in_plane, chans)), shape((STATE // in_plane, chans + LANES))),
        name="plane",
    )(got)
    planes = lax.axis_size("sp_0")
    lower = [lax.ppermute(total, "sp_0", [(i, i + s) for i in range(planes - s)]) for s in (1, 2, 3)]
    back = pl.pallas_call(planes_kernel, out_shape=shape((STATE, chans), BF16), name="planes")(pin, pdec, *lower)
    incoming = lax.all_to_all(back, PLANE, split_axis=0, concat_axis=0, tiled=True)

    step = 512
    half = lax.axis_index("tp").astype(jnp.int32).reshape(1)
    own, other = pl.pallas_call(
        project_kernel,
        grid=(dim // step,),
        in_specs=[
            pl.BlockSpec(memory_space=pltpu.SMEM),
            whole((length, chans)), whole((STATE, chans)), whole((length, vecs)), whole((length, LANES)),
            whole((length, chans)), whole((1, chans)), pl.BlockSpec((chans, step), lambda n: (0, n)),
        ],
        out_specs=(pl.BlockSpec((rows, step), lambda n: (0, n)), pl.BlockSpec((rows, step), lambda n: (0, n))),
        out_shape=(shape((rows, dim)), shape((rows, dim), BF16)),
        scratch_shapes=[pltpu.VMEM((length, chans), BF16), pltpu.VMEM((length, step), F32)],
        name="project",
    )(half, near, incoming, rv, cum, output_gate_input, grouped_norm_gain[None], mixer_output_weight)
    partner = lax.ppermute(other, "tp", [(0, 1), (1, 0)])

    residual, normed, outgoing = pl.pallas_call(
        dispatch_kernel,
        out_shape=(shape((rows, dim), BF16), shape((rows, dim), BF16), shape((experts * WIDE, wide), BF16)),
        scratch_shapes=[pltpu.VMEM((experts * WIDE, 2 * rows), BF16)],
        name="dispatch",
    )(own, partner, stream, expert_norm_gain[None], chosen_expert_index)
    arrived = lax.all_to_all(outgoing, SP_TP, split_axis=0, concat_axis=0, tiled=True)

    part = 128
    base = pl.pallas_call(
        shared_kernel,
        grid=(hidden // part,),
        in_specs=[
            whole((rows, dim)), whole((rows, dim)), pl.BlockSpec((dim, part), lambda n: (0, n)),
            pl.BlockSpec((dim, part), lambda n: (0, n)), pl.BlockSpec((part, dim), lambda n: (n, 0)),
        ],
        out_specs=whole((rows, dim)),
        out_shape=shape((rows, dim)),
        cost_estimate=pl.CostEstimate(flops=800_000_000, transcendentals=70_000, bytes_accessed=8_000_000),
        name="shared",
    )(normed, residual, common_gate_weight, common_up_weight, common_down_weight)

    tall = 256
    inner = routed_gate_weight.shape[2]
    served = pl.pallas_call(
        expert_kernel,
        grid=(experts * WIDE // tall,),
        in_specs=[
            pl.BlockSpec((tall, wide), lambda m: (m, 0)),
            pl.BlockSpec((None, dim, inner), lambda m: (0, 0, 0)),
            pl.BlockSpec((None, dim, inner), lambda m: (0, 0, 0)),
            pl.BlockSpec((None, inner, dim), lambda m: (0, 0, 0)),
        ],
        out_specs=pl.BlockSpec((tall, wide), lambda m: (m, 0)),
        out_shape=shape((experts * WIDE, wide), BF16),
        scratch_shapes=[pltpu.VMEM((tall, dim), BF16)],
        name="experts",
    )(arrived, routed_gate_weight, routed_up_weight, routed_down_weight)
    returned = lax.all_to_all(served, SP_TP, split_axis=0, concat_axis=0, tiled=True)

    fanout = chosen_expert_index.shape[1]
    return pl.pallas_call(
        combine_kernel,
        grid=(3,),
        in_specs=[
            pl.BlockSpec((experts * WIDE, wide // 3), lambda q: (0, q)),
            whole((rows, dim)), whole((rows, fanout)), whole((rows, fanout)),
        ],
        out_specs=whole((rows, dim)),
        out_shape=shape((rows, dim), BF16),
        scratch_shapes=[pltpu.VMEM((4 * rows, experts * WIDE), BF16), pltpu.VMEM((rows, wide // 3), F32)],
        name="combine",
    )(returned, base, chosen_expert_index, chosen_expert_weight)


def solution(mesh):
    split = Mesh(mesh.devices.reshape(4, 4, 4, mesh.shape["tp"]), ("sp_0", "sp_1", "sp_2", "tp"))
    return jax.shard_map(
        on_device,
        mesh=split,
        in_specs=(
            P(SP_TP, None),
            P(SP, "tp"),
            P(SP, "tp"),
            P(SP, "tp"),
            P(SP, "tp"),
            P(SP, "tp"),
            P(SP, "tp"),
            P(None, "tp"),
            P(None, "tp"),
            P(None, "tp"),
            P("tp"),
            P("tp"),
            P("tp"),
            P("tp"),
            P("tp", None),
            P(),
            P(SP_TP, None),
            P(SP_TP, None),
            P(SP_TP, None, None),
            P(SP_TP, None, None),
            P(SP_TP, None, None),
            P(),
            P(),
            P(),
        ),
        out_specs=P(SP_TP, None),
        check_vma=False,
    )
```

```python
import jax
import jax.numpy as jnp
from jax import lax
from jax.experimental import pallas as pl
from jax.experimental.pallas import tpu as pltpu
from jax.sharding import Mesh
from jax.sharding import PartitionSpec as P

HEAD_DIM = 64
STATE = 128
BLK = 128
HEAD = 16
LANES = 128
SLOTS = 6
WIDE = 8
SP = ("sp_0", "sp_1", "sp_2")
PLANE = ("sp_1", "sp_2")
SP_TP = ("sp_0", "sp_1", "sp_2", "tp")
F32 = jnp.float32
BF16 = jnp.bfloat16


def mm(a, b, dims=((1,), (0,)), precision=None):
    return lax.dot_general(a, b, (dims, ((), ())), precision=precision, preferred_element_type=F32)


def iota(shape, dim):
    return lax.broadcasted_iota(jnp.int32, shape, dim)


def head_lanes(width):
    return jnp.where(iota((LANES, width), 1) // HEAD_DIM == iota((LANES, width), 0), 1.0, 0.0).astype(BF16)


def spread(values, lanes):
    high = values.astype(BF16)
    low = (values - high.astype(F32)).astype(BF16)
    return mm(high, lanes) + mm(low, lanes)


def silu(v):
    return v * (1.0 / (1.0 + jnp.exp(-v)))


def onchip(count):
    return [pl.BlockSpec(memory_space=pltpu.VMEM)] * count


def offchip(count):
    return [pl.BlockSpec(memory_space=pltpu.HBM)] * count


def stay(*arrays):
    return [pltpu.with_memory_space_constraint(array, pltpu.HBM) for array in arrays]


def room(mebibytes):
    return pltpu.CompilerParams(vmem_limit_bytes=mebibytes << 20)


def whole(shape):
    return pl.BlockSpec(shape, lambda *_: (0,) * len(shape))


def fetch(pairs, sems):
    copies = [pltpu.make_async_copy(src, dst, sems.at[i]) for i, (src, dst) in enumerate(pairs)]
    for copy in copies:
        copy.start()
    return copies


def rim_kernel(x_ref, b_ref, c_ref, out_ref, sems):
    start, pairs = 0, []
    for ref in (x_ref, b_ref, c_ref):
        rows, size = ref.shape
        pairs.append((ref.at[rows - 8 : rows, :], out_ref.at[:, start : start + size]))
        start += size
    for copy in fetch(pairs, sems):
        copy.wait()


def filtered(ext_ref, taps, lanes, first, count):
    total = taps[0:1] * ext_ref[first : first + count, lanes]
    for k in range(1, 4):
        total = total + taps[k : k + 1] * ext_ref[first + k : first + k + count, lanes]
    return silu(total)


def front_kernel(x_hbm, b_hbm, c_hbm, dt_hbm, pld_hbm, tx_hbm, tb_hbm, tc_hbm, bias_hbm, rate_hbm,
                 sig_ref, wv_ref, rv_ref, cum_ref, rows_ref, dtv_ref, s0_ref, s1_ref, begin_ref, taps_ref,
                 x_ref, b_ref, c_ref, dt_ref, pld_ref, tx_ref, tb_ref, tc_ref, bias_ref, rate_ref, ext_ref, wide_ref, sems):
    length, chans = x_ref.shape
    vecs = b_ref.shape[1]
    heads = dt_ref.shape[0]
    groups = vecs // STATE
    width = chans // groups
    copies = fetch((
        (bias_hbm, bias_ref), (rate_hbm, rate_ref), (dt_hbm, dt_ref), (pld_hbm, pld_ref), (tx_hbm, tx_ref), (tb_hbm, tb_ref),
        (tc_hbm, tc_ref), (b_hbm, b_ref), (c_hbm, c_ref), (x_hbm, x_ref),
    ), sems)
    for copy in copies[0:4]:
        copy.wait()
    wide_ref[...] = jnp.zeros_like(wide_ref)
    wide_ref[0:1, 0:heads] = bias_ref[...]
    wide_ref[1:2, 0:heads] = rate_ref[...]
    columns = wide_ref[:, 0:LANES].T
    v = dt_ref[...].astype(F32) + columns[0:heads, 0:1]
    step = jnp.maximum(v, 0.0) + jnp.log(1.0 + jnp.exp(-jnp.abs(v)))
    logs = pld_ref[...] - columns[0:heads, 1:2] * step
    upper = jnp.where(iota((length, length), 0) <= iota((length, length), 1), 1.0, 0.0)
    sums = mm(logs, upper, precision=lax.Precision.HIGHEST)
    rows_ref[...] = sums
    wide_ref[0:heads, :] = step
    dtv_ref[...] = wide_ref[...].T
    wide_ref[0:heads, :] = sums
    cum = wide_ref[...].T
    cum_ref[...] = cum
    half_end, end = cum[BLK - 1 : BLK], cum[length - 1 : length]
    ends = jnp.where(iota((length, LANES), 0) < BLK, half_end, end)
    weights = jnp.where(iota((length, LANES), 0) < HEAD, 0.0, dtv_ref[...] * jnp.exp(ends - cum))
    scale = spread(weights, head_lanes(chans))
    for copy in copies[4:7]:
        copy.wait()
    taps_ref[...] = jnp.zeros_like(taps_ref)
    sources = (
        (b_ref, tb_ref, chans, vecs, wv_ref, copies[7]), (c_ref, tc_ref, chans + vecs, vecs, rv_ref, copies[8]),
        (x_ref, tx_ref, 0, chans, sig_ref, copies[9]),
    )
    ext_ref[0:8, :] = jnp.zeros((8, ext_ref.shape[1]), F32)
    for src, taps, start, size, dst, copy in sources:
        taps_ref[0:4, start : start + size] = taps[...].astype(F32)
        copy.wait()
        ext_ref[8 : 8 + length, start : start + size] = src[...].astype(F32)
        begin_ref[:, start : start + size] = src[0:HEAD, :].astype(F32)
        for at in range(0, size, 256):
            lanes = slice(start + at, start + at + 256)
            dst[:, at : at + 256] = filtered(ext_ref, taps_ref[:, lanes], lanes, 5, length).astype(dst.dtype)
    for g in range(groups):
        part = slice(g * width, (g + 1) * width)
        vec = slice(g * STATE, (g + 1) * STATE)
        scaled = (sig_ref[:, part] * scale[:, part]).astype(BF16)
        s0_ref[:, part] = mm(wv_ref[0:BLK, vec], scaled[0:BLK], ((0,), (0,)))
        s1_ref[:, part] = mm(wv_ref[BLK:length, vec], scaled[BLK:length], ((0,), (0,)))


def head_kernel(rim_ref, begin_ref, taps_ref, siga_ref, wva_ref, rva_ref, cum_ref, dtv_ref, s0a_ref, s1_ref,
                sig_ref, wv_ref, rv_ref, s0_ref, send_ref, ext_ref):
    length, chans = siga_ref.shape
    vecs = wva_ref.shape[1]
    groups = vecs // STATE
    width = chans // groups
    ext_ref[0:8, :] = rim_ref[...].astype(F32)
    ext_ref[8 : 8 + HEAD, :] = begin_ref[...]
    for start, size, old, new in ((0, chans, siga_ref, sig_ref), (chans, vecs, wva_ref, wv_ref), (chans + vecs, vecs, rva_ref, rv_ref)):
        lanes = slice(start, start + size)
        new[0:HEAD, :] = filtered(ext_ref, taps_ref[:, lanes], lanes, 5, HEAD).astype(new.dtype)
        new[HEAD:, :] = old[HEAD:, :]
    half_end, end = cum_ref[BLK - 1 : BLK, :], cum_ref[length - 1 : length, :]
    lanes = head_lanes(chans)
    scale = spread(dtv_ref[0:HEAD, :] * jnp.exp(half_end - cum_ref[0:HEAD, :]), lanes)
    passing = spread(jnp.broadcast_to(jnp.exp(end - half_end), (8, LANES)), lanes)[0:1]
    scaled = (sig_ref[0:HEAD, :] * scale).astype(BF16)
    for g in range(groups):
        part = slice(g * width, (g + 1) * width)
        first = s0a_ref[:, part] + mm(wv_ref[0:HEAD, g * STATE : (g + 1) * STATE], scaled[:, part], ((0,), (0,)))
        s0_ref[:, part] = first
        send_ref[:, part] = (first * passing[:, part] + s1_ref[:, part]).astype(BF16)
    high = end.astype(BF16).astype(F32)
    mid = (end - high).astype(BF16).astype(F32)
    low = (end - high - mid).astype(BF16).astype(F32)
    row = iota((STATE, LANES), 0) % 8
    send_ref[:, chans : chans + LANES] = jnp.where(
        row == 0, high, jnp.where(row == 1, mid, jnp.where(row == 2, low, 0.0))
    ).astype(BF16)


def plane_kernel(got_ref, pin_ref, pdec_ref, send_ref):
    count = got_ref.shape[0] // 8
    chans = got_ref.shape[1] - LANES
    logs = jnp.sum(got_ref[:, chans:].astype(F32).reshape(count, 8, LANES), axis=1)
    lanes = head_lanes(chans)
    decay = spread(jnp.exp(logs), lanes)
    state = jnp.zeros((8, chans), F32)
    sofar = jnp.zeros((1, LANES), F32)
    before = []
    for i in range(count):
        pin_ref[8 * i : 8 * i + 8, :] = state
        before.append(sofar)
        state = state * decay[i : i + 1] + got_ref[8 * i : 8 * i + 8, 0:chans].astype(F32)
        sofar = sofar + logs[i : i + 1]
    pdec_ref[...] = spread(jnp.exp(jnp.concatenate(before, axis=0)), lanes)
    send_ref[:, 0:chans] = state
    send_ref[:, chans:] = jnp.broadcast_to(sofar, (8, LANES))


def planes_kernel(pin_ref, pdec_ref, one_ref, two_ref, three_ref, out_ref):
    chans = pin_ref.shape[1]
    count = pin_ref.shape[0] // 8
    lanes = head_lanes(chans)
    near = spread(jnp.exp(one_ref[:, chans:]), lanes)
    far = spread(jnp.exp(two_ref[:, chans:]), lanes)
    state = one_ref[:, 0:chans] + near * (two_ref[:, 0:chans] + far * three_ref[:, 0:chans])
    for i in range(0, count, 2):
        pair = [pin_ref[8 * k : 8 * k + 8, :] + state * pdec_ref[k : k + 1, :] for k in (i, i + 1)]
        out_ref[8 * i : 8 * i + 16, :] = jnp.concatenate(pair, axis=0).astype(BF16)


def near_kernel(sig_ref, wv_ref, rv_ref, cum_ref, rows_ref, dtv_ref, s0_ref, direct_ref, y_ref, pad_ref):
    length, chans = sig_ref.shape
    heads = direct_ref.shape[1]
    groups = wv_ref.shape[1] // STATE
    width = chans // groups
    lanes = head_lanes(chans)
    cum = cum_ref[...]
    cum_rows = rows_ref[...]
    pad_ref[...] = jnp.zeros_like(pad_ref)
    pad_ref[:, 0:heads] = jnp.broadcast_to(direct_ref[...], (8, heads))
    direct = spread(pad_ref[...], lanes)[0:1]
    scaled = (sig_ref[...] * spread(dtv_ref[...], lanes)).astype(BF16)
    causal = iota((BLK, BLK), 0) >= iota((BLK, BLK), 1)
    left = iota((BLK, LANES), 1) < HEAD_DIM
    into = spread(jnp.exp(cum[BLK:length] - cum[BLK - 1 : BLK]), lanes)
    for b in range(length // BLK):
        rows = slice(b * BLK, (b + 1) * BLK)
        for g in range(groups):
            vec = slice(g * STATE, (g + 1) * STATE)
            part = slice(g * width, (g + 1) * width)
            products = mm(rv_ref[rows, vec], wv_ref[rows, vec], ((1,), (1,)))
            if b == 1:
                carried = mm(rv_ref[rows, vec], s0_ref[:, part].astype(BF16)) * into[:, part]
            for j in range(width // LANES):
                at = g * width + j * LANES
                mats = []
                for h in (at // HEAD_DIM, at // HEAD_DIM + 1):
                    gap = cum[rows, h : h + 1] - cum_rows[h : h + 1, rows]
                    mats.append((products * jnp.exp(jnp.where(causal, gap, -1e30))).astype(BF16))
                pair = scaled[rows, at : at + LANES]
                zero = jnp.zeros_like(pair)
                stacked = jnp.concatenate([jnp.where(left, pair, zero), jnp.where(left, zero, pair)], axis=0)
                out = mm(jnp.concatenate(mats, axis=1), stacked)
                out = out + direct[:, at : at + LANES] * sig_ref[rows, at : at + LANES]
                if b == 1:
                    out = out + carried[:, j * LANES : (j + 1) * LANES]
                y_ref[rows, at : at + LANES] = out


def project_kernel(half_ref, y_ref, state_ref, rv_ref, cum_ref, gate_hbm, gain_hbm, w_hbm, own_ref, other_ref,
                   gate_ref, gain_ref, w_ref, mix_ref, res_ref, sems):
    length, chans = y_ref.shape
    groups = rv_ref.shape[1] // STATE
    width = chans // groups
    rows = own_ref.shape[0]
    dim = own_ref.shape[1]
    parts = 4
    pairs = [(gate_hbm, gate_ref), (gain_hbm, gain_ref)]
    for k in range(parts):
        part = pl.ds(k * (dim // parts), dim // parts)
        pairs.append((w_hbm.at[:, part], w_ref.at[:, part]))
    copies = fetch(pairs, sems)
    scale = spread(jnp.exp(cum_ref[...]), head_lanes(chans))
    for g in range(groups):
        part = slice(g * width, (g + 1) * width)
        far = mm(rv_ref[:, g * STATE : (g + 1) * STATE], state_ref[:, part])
        inner = y_ref[:, part] + far * scale[:, part]
        if g == 0:
            copies[0].wait()
            copies[1].wait()
        gated = inner * silu(gate_ref[:, part].astype(F32))
        mean = jnp.sum(gated * gated, axis=1, keepdims=True) * (1.0 / width)
        mix_ref[:, part] = (gated * lax.rsqrt(mean + 1e-06) * gain_ref[:, part]).astype(BF16)
    half = half_ref[0]
    for k in range(parts):
        part = slice(k * (dim // parts), (k + 1) * (dim // parts))
        copies[2 + k].wait()
        res_ref[...] = mm(mix_ref[...], w_ref[:, part])
        own_ref[:, part] = res_ref[pl.ds(pl.multiple_of(half * rows, rows), rows), :]
        other_ref[:, part] = res_ref[pl.ds(pl.multiple_of((1 - half) * rows, rows), rows), :].astype(BF16)


def slot_table(chosen, experts):
    count = chosen.shape[1]
    expert = iota((experts, count), 0)
    named = jnp.zeros((experts, count), F32)
    for k in range(chosen.shape[0]):
        named = named + jnp.where(chosen[k : k + 1, :] == expert, 1.0, 0.0)
    earlier = jnp.where(iota((count, count), 0) < iota((count, count), 1), 1.0, 0.0).astype(BF16)
    return named * (mm(named.astype(BF16), earlier) + 1.0)


def expert_rows(experts):
    return jnp.where(iota((experts * WIDE, experts), 0) // WIDE == iota((experts * WIDE, experts), 1), 1.0, 0.0).astype(BF16)


def dispatch_kernel(own_ref, got_ref, stream_hbm, gain_hbm, chosen_ref, residual_ref, normed_ref, out_ref,
                    stream_ref, gain_ref, both_ref, sems):
    rows, dim = own_ref.shape
    third = out_ref.shape[1] // 3
    experts = out_ref.shape[0] // WIDE
    copies = fetch(((stream_hbm, stream_ref), (gain_hbm, gain_ref)), sems)
    table = slot_table(chosen_ref[...], experts)
    slots = mm(expert_rows(experts), table.astype(BF16))
    place = (iota(slots.shape, 0) % WIDE).astype(F32)
    both_ref[:, 0:rows] = jnp.where(slots == place + 1.0, 1.0, 0.0).astype(BF16)
    for q in range(3):
        tail = jnp.where((place >= 6.0) & (slots == 3.0 * place + (q - 17.0)), 1.0, 0.0)
        both_ref[:, rows * (q + 1) : rows * (q + 2)] = tail.astype(BF16)
    for copy in copies:
        copy.wait()
    residual = (stream_ref[...].astype(F32) + own_ref[...] + got_ref[...].astype(F32)).astype(BF16)
    residual_ref[...] = residual
    wide = residual.astype(F32)
    mean = jnp.sum(wide * wide, axis=1, keepdims=True) * (1.0 / dim)
    normed_ref[...] = (wide * lax.rsqrt(mean + 1e-06) * gain_ref[...]).astype(BF16)
    main = both_ref[:, 0:rows]
    for q in range(3):
        mats = jnp.concatenate([main, both_ref[:, rows * (q + 1) : rows * (q + 2)]], axis=1)
        source = jnp.concatenate([normed_ref[:, q * third : (q + 1) * third], normed_ref[:, 3 * third :]], axis=0)
        out_ref[:, q * third : (q + 1) * third] = mm(mats, source).astype(BF16)


def shared_kernel(normed_ref, residual_ref, gate_ref, up_ref, down_ref, chosen_ref, weight_ref, out_ref, mats_ref):
    @pl.when(pl.program_id(0) == 0)
    def _():
        out_ref[...] = residual_ref[...].astype(F32)
        rows = normed_ref.shape[0]
        experts = mats_ref.shape[1] // WIDE
        chosen = chosen_ref[...]
        expert = iota((experts, rows), 0)
        weights = jnp.zeros((experts, rows), F32)
        for k in range(chosen.shape[0]):
            weights = weights + jnp.where(chosen[k : k + 1, :] == expert, weight_ref[k : k + 1, :], 0.0)
        lanes = expert_rows(experts)
        slots = mm(slot_table(chosen, experts).T.astype(BF16), lanes, ((1,), (1,)))
        spread_weights = mm(weights.T.astype(BF16), lanes, ((1,), (1,)))
        place = (iota(slots.shape, 1) % WIDE).astype(F32)
        mats_ref[0:rows, :] = jnp.where(slots == place + 1.0, spread_weights, 0.0).astype(BF16)
        for k in range(3):
            hit = (place >= 6.0) & (slots == 3.0 * place + (k - 17.0))
            mats_ref[rows * (k + 1) : rows * (k + 2), :] = jnp.where(hit, spread_weights, 0.0).astype(BF16)

    normed = normed_ref[...]
    hidden = (silu(mm(normed, gate_ref[...])) * mm(normed, up_ref[...])).astype(BF16)
    out_ref[...] += mm(hidden, down_ref[...])


def expert_kernel(x_ref, gate_ref, up_ref, down_ref, out_hbm, full_ref, out_ref, sems):
    total, wide = x_ref.shape
    third = wide // 3
    rows = out_ref.shape[1]
    row, col = iota((LANES, LANES), 0), iota((LANES, LANES), 1)
    same = row // WIDE == col // WIDE
    r, c = row % WIDE, col % WIDE
    unpack = [jnp.where(same & (c >= 6) & (r == 3 * (c - 6) + q), 1.0, 0.0).astype(BF16) for q in range(3)]
    pack = [jnp.where(same & (r >= 6) & (c == 3 * (r - 6) + q), 1.0, 0.0).astype(BF16) for q in range(3)]
    unpack, pack = jnp.concatenate(unpack, axis=1), jnp.concatenate(pack, axis=0)
    within = iota((LANES, third), 0) % WIDE < SLOTS
    copies = []
    for n in range(total // rows):
        base = n * rows
        full_ref[:, 0:wide] = x_ref[base : base + rows, :]
        for at in range(0, rows, LANES):
            pieces = [x_ref[base + at : base + at + LANES, q * third : (q + 1) * third] for q in range(3)]
            full_ref[at : at + LANES, wide:] = mm(unpack, jnp.concatenate(pieces, axis=0)).astype(BF16)
        full = full_ref[...]
        hidden = (silu(mm(full, gate_ref[...])) * mm(full, up_ref[...])).astype(BF16)
        tail = mm(hidden, down_ref[:, wide:]).astype(BF16)
        packed = [mm(pack, tail[at : at + LANES]) for at in range(0, rows, LANES)]
        for q in range(3):
            part = slice(q * third, (q + 1) * third)
            result = mm(hidden, down_ref[:, part])
            for k, at in enumerate(range(0, rows, LANES)):
                extra = packed[k][q * LANES : (q + 1) * LANES]
                out_ref[n, at : at + LANES, part] = jnp.where(within, result[at : at + LANES], extra).astype(BF16)
        copy = pltpu.make_async_copy(out_ref.at[n], out_hbm.at[base : base + rows, :], sems.at[n])
        copy.start()
        copies.append(copy)
    for copy in copies:
        copy.wait()


def combine_kernel(got_ref, base_hbm, mats_hbm, out_ref, base_ref, mats_ref, sems):
    rows, dim = base_ref.shape
    third = got_ref.shape[1] // 3
    copies = fetch(((mats_hbm, mats_ref), (base_hbm, base_ref)), sems)
    tail = jnp.zeros((rows, third), F32)
    copies[0].wait()
    for q in range(3):
        part = slice(q * third, (q + 1) * third)
        got = got_ref[:, part]
        main = mm(mats_ref[0:rows, :], got)
        tail = tail + mm(mats_ref[rows * (q + 1) : rows * (q + 2), :], got)
        if q == 0:
            copies[1].wait()
        out_ref[:, part] = (base_ref[:, part] + main).astype(BF16)
    out_ref[:, 3 * third :] = (base_ref[:, 3 * third :] + tail).astype(BF16)


def shape(dims, dtype=F32):
    return jax.ShapeDtypeStruct(dims, dtype)


def on_device(
    stream,
    head_input_signal,
    write_input_vectors,
    read_input_vectors,
    output_gate_input,
    step_size_input,
    position_log_decay,
    signal_filter_taps,
    write_filter_taps,
    read_filter_taps,
    step_size_bias,
    head_decay_rate,
    head_direct_term,
    grouped_norm_gain,
    mixer_output_weight,
    expert_norm_gain,
    chosen_expert_index,
    chosen_expert_weight,
    routed_gate_weight,
    routed_up_weight,
    routed_down_weight,
    common_gate_weight,
    common_up_weight,
    common_down_weight,
):
    length, chans = head_input_signal.shape
    vecs = write_input_vectors.shape[1]
    rows, dim = stream.shape
    hidden = common_gate_weight.shape[1]
    experts = lax.axis_size(SP_TP)
    wide = dim * SLOTS // WIDE

    heads = step_size_input.shape[1]
    devices = lax.axis_size(SP)
    rim = pl.pallas_call(
        rim_kernel,
        in_specs=offchip(3),
        out_specs=onchip(1)[0],
        out_shape=shape((8, chans + 2 * vecs), BF16),
        scratch_shapes=[pltpu.SemaphoreType.DMA((3,))],
        compiler_params=room(2),
        name="rim",
    )(*stay(head_input_signal, write_input_vectors, read_input_vectors))
    rim = lax.ppermute(rim, SP, [(i, i + 1) for i in range(devices - 1)])
    signal, write_rows, read_rows, cum, cum_rows, dtv, first, second, begin, taps = pl.pallas_call(
        front_kernel,
        in_specs=offchip(10),
        out_specs=tuple(onchip(10)),
        out_shape=(
            shape((length, chans)), shape((length, vecs), BF16), shape((length, vecs), BF16), shape((length, LANES)),
            shape((heads, length)), shape((length, LANES)), shape((STATE, chans)), shape((STATE, chans)),
            shape((HEAD, chans + 2 * vecs)), shape((8, chans + 2 * vecs)),
        ),
        scratch_shapes=[
            pltpu.VMEM((length, chans), BF16), pltpu.VMEM((length, vecs), BF16), pltpu.VMEM((length, vecs), BF16),
            pltpu.VMEM((heads, length), BF16), pltpu.VMEM((heads, length), F32),
            pltpu.VMEM((4, chans), BF16), pltpu.VMEM((4, vecs), BF16), pltpu.VMEM((4, vecs), BF16),
            pltpu.VMEM((1, heads), F32), pltpu.VMEM((1, heads), F32),
            pltpu.VMEM((length + 8, chans + 2 * vecs), F32), pltpu.VMEM((LANES, length), F32),
            pltpu.SemaphoreType.DMA((10,)),
        ],
        cost_estimate=pl.CostEstimate(flops=800_000_000, transcendentals=1_000_000, bytes_accessed=4_000_000),
        compiler_params=room(14),
        name="front",
    )(*stay(
        head_input_signal, write_input_vectors, read_input_vectors, step_size_input.T, position_log_decay.T,
        signal_filter_taps, write_filter_taps, read_filter_taps, step_size_bias[None], head_decay_rate[None],
    ))
    sig, wv, rv, s0, send = pl.pallas_call(
        head_kernel,
        in_specs=onchip(10),
        out_specs=tuple(onchip(5)),
        out_shape=(
            shape((length, chans)), shape((length, vecs), BF16), shape((length, vecs), BF16),
            shape((STATE, chans)), shape((STATE, chans + LANES), BF16),
        ),
        scratch_shapes=[pltpu.VMEM((HEAD + 8, chans + 2 * vecs), F32)],
        compiler_params=room(8),
        name="head",
    )(rim, begin, taps, signal, write_rows, read_rows, cum, dtv, first, second)
    in_plane = lax.axis_size(PLANE)
    got = lax.all_to_all(send, PLANE, split_axis=0, concat_axis=0, tiled=True)
    near = pl.pallas_call(
        near_kernel,
        in_specs=onchip(8),
        out_specs=onchip(1)[0],
        out_shape=shape((length, chans)),
        scratch_shapes=[pltpu.VMEM((8, LANES), F32)],
        cost_estimate=pl.CostEstimate(flops=400_000_000, transcendentals=1_000_000, bytes_accessed=4_000_000),
        compiler_params=room(12),
        name="near",
    )(sig, wv, rv, cum, cum_rows, dtv, s0, head_direct_term[None])
    pin, pdec, total = pl.pallas_call(
        plane_kernel,
        in_specs=onchip(1),
        out_specs=tuple(onchip(3)),
        out_shape=(shape((STATE, chans)), shape((in_plane, chans)), shape((STATE // in_plane, chans + LANES))),
        compiler_params=room(6),
        name="plane",
    )(got)
    planes = lax.axis_size("sp_0")
    lower = [lax.ppermute(total, "sp_0", [(i, i + s) for i in range(planes - s)]) for s in (1, 2, 3)]
    back = pl.pallas_call(
        planes_kernel,
        in_specs=onchip(5),
        out_specs=onchip(1)[0],
        out_shape=shape((STATE, chans), BF16),
        compiler_params=room(6),
        name="planes",
    )(pin, pdec, *lower)
    incoming = lax.all_to_all(back, PLANE, split_axis=0, concat_axis=0, tiled=True)

    half = lax.axis_index("tp").astype(jnp.int32).reshape(1)
    own, other = pl.pallas_call(
        project_kernel,
        in_specs=[pl.BlockSpec(memory_space=pltpu.SMEM)] + onchip(4) + offchip(3),
        out_specs=tuple(onchip(2)),
        out_shape=(shape((rows, dim)), shape((rows, dim), BF16)),
        scratch_shapes=[
            pltpu.VMEM((length, chans), BF16), pltpu.VMEM((1, chans), F32), pltpu.VMEM((chans, dim), BF16),
            pltpu.VMEM((length, chans), BF16), pltpu.VMEM((length, dim // 4), F32), pltpu.SemaphoreType.DMA((6,)),
        ],
        compiler_params=room(16),
        name="project",
    )(half, near, incoming, rv, cum, *stay(output_gate_input, grouped_norm_gain[None], mixer_output_weight))
    partner = lax.ppermute(other, "tp", [(0, 1), (1, 0)])

    chosen = chosen_expert_index.T
    residual, normed, outgoing = pl.pallas_call(
        dispatch_kernel,
        in_specs=onchip(2) + offchip(2) + onchip(1),
        out_specs=tuple(onchip(3)),
        out_shape=(shape((rows, dim), BF16), shape((rows, dim), BF16), shape((experts * WIDE, wide), BF16)),
        scratch_shapes=[
            pltpu.VMEM((rows, dim), BF16), pltpu.VMEM((1, dim), F32), pltpu.VMEM((experts * WIDE, 4 * rows), BF16),
            pltpu.SemaphoreType.DMA((2,)),
        ],
        compiler_params=room(14),
        name="dispatch",
    )(own, partner, *stay(stream, expert_norm_gain[None]), chosen)
    arrived = lax.all_to_all(outgoing, SP_TP, split_axis=0, concat_axis=0, tiled=True)

    part = 128
    fanout = chosen.shape[0]
    base, mats = pl.pallas_call(
        shared_kernel,
        grid=(hidden // part,),
        in_specs=[
            whole((rows, dim)), whole((rows, dim)), pl.BlockSpec((dim, part), lambda n: (0, n)),
            pl.BlockSpec((dim, part), lambda n: (0, n)), pl.BlockSpec((part, dim), lambda n: (n, 0)),
            whole((fanout, rows)), whole((fanout, rows)),
        ],
        out_specs=(whole((rows, dim)), whole((4 * rows, experts * WIDE))),
        out_shape=(pltpu.HBM((rows, dim), F32), pltpu.HBM((4 * rows, experts * WIDE), BF16)),
        cost_estimate=pl.CostEstimate(flops=800_000_000, transcendentals=70_000, bytes_accessed=8_000_000),
        compiler_params=room(16),
        name="shared",
    )(normed, residual, *stay(common_gate_weight, common_up_weight, common_down_weight), chosen, chosen_expert_weight.T)

    chunks = 2
    tall = experts * WIDE // chunks
    served = pl.pallas_call(
        expert_kernel,
        in_specs=onchip(4),
        out_specs=offchip(1)[0],
        out_shape=pltpu.HBM((experts * WIDE, wide), BF16),
        scratch_shapes=[pltpu.VMEM((tall, dim), BF16), pltpu.VMEM((chunks, tall, wide), BF16), pltpu.SemaphoreType.DMA((chunks,))],
        compiler_params=room(24),
        name="experts",
    )(arrived, routed_gate_weight[0], routed_up_weight[0], routed_down_weight[0])
    returned = lax.all_to_all(served, SP_TP, split_axis=0, concat_axis=0, tiled=True)

    return pl.pallas_call(
        combine_kernel,
        in_specs=onchip(1) + offchip(2),
        out_specs=onchip(1)[0],
        out_shape=shape((rows, dim), BF16),
        scratch_shapes=[pltpu.VMEM((rows, dim), F32), pltpu.VMEM((4 * rows, experts * WIDE), BF16), pltpu.SemaphoreType.DMA((2,))],
        compiler_params=room(12),
        name="combine",
    )(returned, *stay(base, mats))


def solution(mesh):
    split = Mesh(mesh.devices.reshape(4, 4, 4, mesh.shape["tp"]), ("sp_0", "sp_1", "sp_2", "tp"))
    return jax.shard_map(
        on_device,
        mesh=split,
        in_specs=(
            P(SP_TP, None),
            P(SP, "tp"),
            P(SP, "tp"),
            P(SP, "tp"),
            P(SP, "tp"),
            P(SP, "tp"),
            P(SP, "tp"),
            P(None, "tp"),
            P(None, "tp"),
            P(None, "tp"),
            P("tp"),
            P("tp"),
            P("tp"),
            P("tp"),
            P("tp", None),
            P(),
            P(SP_TP, None),
            P(SP_TP, None),
            P(SP_TP, None, None),
            P(SP_TP, None, None),
            P(SP_TP, None, None),
            P(),
            P(),
            P(),
        ),
        out_specs=P(SP_TP, None),
        check_vma=False,
    )
```

```python
import jax
import jax.numpy as jnp
from jax import lax
from jax.experimental import pallas as pl
from jax.experimental.pallas import tpu as pltpu
from jax.sharding import Mesh
from jax.sharding import PartitionSpec as P

HEAD_DIM = 64
STATE = 128
BLK = 128
HEAD = 16
LANES = 128
SLOTS = 6
WIDE = 8
SP = ("sp_0", "sp_1", "sp_2")
PLANE = ("sp_1", "sp_2")
SP_TP = ("sp_0", "sp_1", "sp_2", "tp")
F32 = jnp.float32
BF16 = jnp.bfloat16


def mm(a, b, dims=((1,), (0,)), precision=None):
    return lax.dot_general(a, b, (dims, ((), ())), precision=precision, preferred_element_type=F32)


def iota(shape, dim):
    return lax.broadcasted_iota(jnp.int32, shape, dim)


def head_lanes(width):
    return jnp.where(iota((LANES, width), 1) // HEAD_DIM == iota((LANES, width), 0), 1.0, 0.0).astype(BF16)


def spread(values, lanes):
    high = values.astype(BF16)
    low = (values - high.astype(F32)).astype(BF16)
    return mm(high, lanes) + mm(low, lanes)


def silu(v):
    return v * (1.0 / (1.0 + jnp.exp(-v)))


def onchip(count):
    return [pl.BlockSpec(memory_space=pltpu.VMEM)] * count


def offchip(count):
    return [pl.BlockSpec(memory_space=pltpu.HBM)] * count


def stay(*arrays):
    return [pltpu.with_memory_space_constraint(array, pltpu.HBM) for array in arrays]


def room(mebibytes):
    return pltpu.CompilerParams(vmem_limit_bytes=mebibytes << 20)


def whole(shape):
    return pl.BlockSpec(shape, lambda *_: (0,) * len(shape))


def fetch(pairs, sems):
    copies = [pltpu.make_async_copy(src, dst, sems.at[i]) for i, (src, dst) in enumerate(pairs)]
    for copy in copies:
        copy.start()
    return copies


def rim_kernel(x_ref, b_ref, c_ref, out_ref, sems):
    start, pairs = 0, []
    for ref in (x_ref, b_ref, c_ref):
        rows, size = ref.shape
        pairs.append((ref.at[rows - 8 : rows, :], out_ref.at[:, start : start + size]))
        start += size
    for copy in fetch(pairs, sems):
        copy.wait()


def filtered(ext_ref, taps, lanes, first, count):
    total = taps[0:1] * ext_ref[first : first + count, lanes]
    for k in range(1, 4):
        total = total + taps[k : k + 1] * ext_ref[first + k : first + k + count, lanes]
    return silu(total)


def front_kernel(x_hbm, b_hbm, c_hbm, dt_hbm, pld_hbm, tx_hbm, tb_hbm, tc_hbm, bias_hbm, rate_hbm,
                 sig_ref, wv_ref, rv_ref, cum_ref, rows_ref, dtv_ref, s0_ref, s1_ref, begin_ref, taps_ref,
                 x_ref, b_ref, c_ref, dt_ref, pld_ref, tx_ref, tb_ref, tc_ref, bias_ref, rate_ref, ext_ref, wide_ref, sems):
    length, chans = x_ref.shape
    vecs = b_ref.shape[1]
    heads = dt_ref.shape[0]
    groups = vecs // STATE
    width = chans // groups
    copies = fetch((
        (bias_hbm, bias_ref), (rate_hbm, rate_ref), (dt_hbm, dt_ref), (pld_hbm, pld_ref), (tx_hbm, tx_ref), (tb_hbm, tb_ref),
        (tc_hbm, tc_ref), (b_hbm, b_ref), (c_hbm, c_ref), (x_hbm, x_ref),
    ), sems)
    for copy in copies[0:4]:
        copy.wait()
    wide_ref[...] = jnp.zeros_like(wide_ref)
    wide_ref[0:1, 0:heads] = bias_ref[...]
    wide_ref[1:2, 0:heads] = rate_ref[...]
    columns = wide_ref[:, 0:LANES].T
    v = dt_ref[...].astype(F32) + columns[0:heads, 0:1]
    step = jnp.maximum(v, 0.0) + jnp.log(1.0 + jnp.exp(-jnp.abs(v)))
    logs = pld_ref[...] - columns[0:heads, 1:2] * step
    upper = jnp.where(iota((length, length), 0) <= iota((length, length), 1), 1.0, 0.0)
    sums = mm(logs, upper, precision=lax.Precision.HIGHEST)
    rows_ref[...] = sums
    wide_ref[0:heads, :] = step
    dtv_ref[...] = wide_ref[...].T
    wide_ref[0:heads, :] = sums
    cum = wide_ref[...].T
    cum_ref[...] = cum
    half_end, end = cum[BLK - 1 : BLK], cum[length - 1 : length]
    ends = jnp.where(iota((length, LANES), 0) < BLK, half_end, end)
    weights = jnp.where(iota((length, LANES), 0) < HEAD, 0.0, dtv_ref[...] * jnp.exp(ends - cum))
    scale = spread(weights, head_lanes(chans))
    for copy in copies[4:7]:
        copy.wait()
    taps_ref[...] = jnp.zeros_like(taps_ref)
    sources = (
        (b_ref, tb_ref, chans, vecs, wv_ref, copies[7]), (c_ref, tc_ref, chans + vecs, vecs, rv_ref, copies[8]),
        (x_ref, tx_ref, 0, chans, sig_ref, copies[9]),
    )
    ext_ref[0:8, :] = jnp.zeros((8, ext_ref.shape[1]), F32)
    for src, taps, start, size, dst, copy in sources:
        taps_ref[0:4, start : start + size] = taps[...].astype(F32)
        copy.wait()
        ext_ref[8 : 8 + length, start : start + size] = src[...].astype(F32)
        begin_ref[:, start : start + size] = src[0:HEAD, :].astype(F32)
        for at in range(0, size, 256):
            lanes = slice(start + at, start + at + 256)
            dst[:, at : at + 256] = filtered(ext_ref, taps_ref[:, lanes], lanes, 5, length).astype(dst.dtype)
    for g in range(groups):
        part = slice(g * width, (g + 1) * width)
        vec = slice(g * STATE, (g + 1) * STATE)
        scaled = (sig_ref[:, part] * scale[:, part]).astype(BF16)
        s0_ref[:, part] = mm(wv_ref[0:BLK, vec], scaled[0:BLK], ((0,), (0,)))
        s1_ref[:, part] = mm(wv_ref[BLK:length, vec], scaled[BLK:length], ((0,), (0,)))


def head_kernel(rim_ref, begin_ref, taps_ref, siga_ref, wva_ref, rva_ref, cum_ref, dtv_ref, s0a_ref, s1_ref,
                sig_ref, wv_ref, rv_ref, s0_ref, send_ref, ext_ref):
    length, chans = siga_ref.shape
    vecs = wva_ref.shape[1]
    groups = vecs // STATE
    width = chans // groups
    ext_ref[0:8, :] = rim_ref[...].astype(F32)
    ext_ref[8 : 8 + HEAD, :] = begin_ref[...]
    for start, size, old, new in ((0, chans, siga_ref, sig_ref), (chans, vecs, wva_ref, wv_ref), (chans + vecs, vecs, rva_ref, rv_ref)):
        lanes = slice(start, start + size)
        new[0:HEAD, :] = filtered(ext_ref, taps_ref[:, lanes], lanes, 5, HEAD).astype(new.dtype)
        new[HEAD:, :] = old[HEAD:, :]
    half_end, end = cum_ref[BLK - 1 : BLK, :], cum_ref[length - 1 : length, :]
    lanes = head_lanes(chans)
    scale = spread(dtv_ref[0:HEAD, :] * jnp.exp(half_end - cum_ref[0:HEAD, :]), lanes)
    passing = spread(jnp.broadcast_to(jnp.exp(end - half_end), (8, LANES)), lanes)[0:1]
    scaled = (sig_ref[0:HEAD, :] * scale).astype(BF16)
    for g in range(groups):
        part = slice(g * width, (g + 1) * width)
        first = s0a_ref[:, part] + mm(wv_ref[0:HEAD, g * STATE : (g + 1) * STATE], scaled[:, part], ((0,), (0,)))
        s0_ref[:, part] = first
        send_ref[:, part] = (first * passing[:, part] + s1_ref[:, part]).astype(BF16)
    high = end.astype(BF16).astype(F32)
    mid = (end - high).astype(BF16).astype(F32)
    low = (end - high - mid).astype(BF16).astype(F32)
    row = iota((STATE, LANES), 0) % 8
    send_ref[:, chans : chans + LANES] = jnp.where(
        row == 0, high, jnp.where(row == 1, mid, jnp.where(row == 2, low, 0.0))
    ).astype(BF16)


def plane_kernel(got_ref, pin_ref, pdec_ref, send_ref):
    count = got_ref.shape[0] // 8
    chans = got_ref.shape[1] - LANES
    logs = jnp.sum(got_ref[:, chans:].astype(F32).reshape(count, 8, LANES), axis=1)
    lanes = head_lanes(chans)
    decay = spread(jnp.exp(logs), lanes)
    state = jnp.zeros((8, chans), F32)
    sofar = jnp.zeros((1, LANES), F32)
    before = []
    for i in range(count):
        pin_ref[8 * i : 8 * i + 8, :] = state
        before.append(sofar)
        state = state * decay[i : i + 1] + got_ref[8 * i : 8 * i + 8, 0:chans].astype(F32)
        sofar = sofar + logs[i : i + 1]
    pdec_ref[...] = spread(jnp.exp(jnp.concatenate(before, axis=0)), lanes)
    for k in range(send_ref.shape[0] // 8):
        send_ref[8 * k : 8 * k + 8, 0:chans] = state
        send_ref[8 * k : 8 * k + 8, chans:] = jnp.broadcast_to(sofar, (8, LANES))


def planes_kernel(plane_ref, pin_ref, pdec_ref, got_ref, out_ref):
    chans = pin_ref.shape[1]
    count = pin_ref.shape[0] // 8
    lanes = head_lanes(chans)
    plane = plane_ref[0]
    state = jnp.zeros((8, chans), F32)
    for k in range(got_ref.shape[0] // 8 - 1):
        rows = slice(8 * k, 8 * k + 8)
        state = jnp.where(k < plane, state * spread(jnp.exp(got_ref[rows, chans:]), lanes) + got_ref[rows, 0:chans], state)
    for i in range(0, count, 2):
        pair = [pin_ref[8 * k : 8 * k + 8, :] + state * pdec_ref[k : k + 1, :] for k in (i, i + 1)]
        out_ref[8 * i : 8 * i + 16, :] = jnp.concatenate(pair, axis=0).astype(BF16)


def near_kernel(sig_ref, wv_ref, rv_ref, cum_ref, rows_ref, dtv_ref, s0_ref, direct_ref, chosen_ref, y_ref, both_hbm, pad_ref, both_ref, sem):
    experts, tokens = both_ref.shape[0] // WIDE, chosen_ref.shape[1]
    slots = mm(expert_rows(experts), slot_table(chosen_ref[...], experts).astype(BF16))
    place = (iota(slots.shape, 0) % WIDE).astype(F32)
    both_ref[:, 0:tokens] = jnp.where(slots == place + 1.0, 1.0, 0.0).astype(BF16)
    for q in range(3):
        tail = jnp.where((place >= 6.0) & (slots == 3.0 * place + (q - 17.0)), 1.0, 0.0)
        both_ref[:, tokens * (q + 1) : tokens * (q + 2)] = tail.astype(BF16)
    copy = pltpu.make_async_copy(both_ref, both_hbm, sem)
    copy.start()
    length, chans = sig_ref.shape
    heads = direct_ref.shape[1]
    groups = wv_ref.shape[1] // STATE
    width = chans // groups
    lanes = head_lanes(chans)
    cum = cum_ref[...]
    cum_rows = rows_ref[...]
    pad_ref[...] = jnp.zeros_like(pad_ref)
    pad_ref[:, 0:heads] = jnp.broadcast_to(direct_ref[...], (8, heads))
    direct = spread(pad_ref[...], lanes)[0:1]
    scaled = (sig_ref[...] * spread(dtv_ref[...], lanes)).astype(BF16)
    causal = iota((BLK, BLK), 0) >= iota((BLK, BLK), 1)
    left = iota((BLK, LANES), 1) < HEAD_DIM
    into = spread(jnp.exp(cum[BLK:length] - cum[BLK - 1 : BLK]), lanes)
    for b in range(length // BLK):
        rows = slice(b * BLK, (b + 1) * BLK)
        for g in range(groups):
            vec = slice(g * STATE, (g + 1) * STATE)
            part = slice(g * width, (g + 1) * width)
            products = mm(rv_ref[rows, vec], wv_ref[rows, vec], ((1,), (1,)))
            if b == 1:
                carried = mm(rv_ref[rows, vec], s0_ref[:, part].astype(BF16)) * into[:, part]
            for j in range(width // LANES):
                at = g * width + j * LANES
                mats = []
                for h in (at // HEAD_DIM, at // HEAD_DIM + 1):
                    gap = cum[rows, h : h + 1] - cum_rows[h : h + 1, rows]
                    mats.append((products * jnp.exp(jnp.where(causal, gap, -1e30))).astype(BF16))
                pair = scaled[rows, at : at + LANES]
                zero = jnp.zeros_like(pair)
                stacked = jnp.concatenate([jnp.where(left, pair, zero), jnp.where(left, zero, pair)], axis=0)
                out = mm(jnp.concatenate(mats, axis=1), stacked)
                out = out + direct[:, at : at + LANES] * sig_ref[rows, at : at + LANES]
                if b == 1:
                    out = out + carried[:, j * LANES : (j + 1) * LANES]
                y_ref[rows, at : at + LANES] = out
    copy.wait()


def project_kernel(half_ref, y_ref, state_ref, rv_ref, cum_ref, gate_hbm, gain_hbm, w_hbm, other_ref, mine_ref, w_ref,
                   gate_ref, gain_ref, mix_ref, sems):
    length, chans = y_ref.shape
    groups = rv_ref.shape[1] // STATE
    width = chans // groups
    rows, dim = other_ref.shape
    parts = 4
    pairs = [(gate_hbm, gate_ref), (gain_hbm, gain_ref)]
    for k in range(parts):
        part = pl.ds(k * (dim // parts), dim // parts)
        pairs.append((w_hbm.at[:, part], w_ref.at[:, part]))
    copies = fetch(pairs, sems)
    scale = spread(jnp.exp(cum_ref[...]), head_lanes(chans))
    for g in range(groups):
        part = slice(g * width, (g + 1) * width)
        far = mm(rv_ref[:, g * STATE : (g + 1) * STATE], state_ref[:, part])
        inner = y_ref[:, part] + far * scale[:, part]
        if g == 0:
            copies[0].wait()
            copies[1].wait()
        gated = inner * silu(gate_ref[:, part].astype(F32))
        mean = jnp.sum(gated * gated, axis=1, keepdims=True) * (1.0 / width)
        mix_ref[:, part] = (gated * lax.rsqrt(mean + 1e-06) * gain_ref[:, part]).astype(BF16)
    half = half_ref[0]
    mine_ref[...] = mix_ref[pl.ds(pl.multiple_of(half * rows, rows), rows), :]
    theirs = mix_ref[pl.ds(pl.multiple_of((1 - half) * rows, rows), rows), :]
    for k in range(parts):
        part = slice(k * (dim // parts), (k + 1) * (dim // parts))
        copies[2 + k].wait()
        other_ref[:, part] = mm(theirs, w_ref[:, part]).astype(BF16)


def own_kernel(mine_ref, w_ref, stream_hbm, own_ref, stream_ref, sem):
    copy = pltpu.make_async_copy(stream_hbm, stream_ref, sem)
    copy.start()
    product = mm(mine_ref[...], w_ref[...])
    copy.wait()
    own_ref[...] = product + stream_ref[...].astype(F32)


def slot_table(chosen, experts):
    count = chosen.shape[1]
    expert = iota((experts, count), 0)
    named = jnp.zeros((experts, count), F32)
    for k in range(chosen.shape[0]):
        named = named + jnp.where(chosen[k : k + 1, :] == expert, 1.0, 0.0)
    earlier = jnp.where(iota((count, count), 0) < iota((count, count), 1), 1.0, 0.0).astype(BF16)
    return named * (mm(named.astype(BF16), earlier) + 1.0)


def expert_rows(experts):
    return jnp.where(iota((experts * WIDE, experts), 0) // WIDE == iota((experts * WIDE, experts), 1), 1.0, 0.0).astype(BF16)


def dispatch_kernel(own_ref, got_ref, gain_hbm, both_hbm, residual_ref, normed_ref, out_ref, gain_ref, both_ref, sems):
    rows, dim = own_ref.shape
    third = out_ref.shape[1] // 3
    copies = fetch(((gain_hbm, gain_ref), (both_hbm, both_ref)), sems)
    residual = (own_ref[...] + got_ref[...].astype(F32)).astype(BF16)
    residual_ref[...] = residual
    wide = residual.astype(F32)
    mean = jnp.sum(wide * wide, axis=1, keepdims=True) * (1.0 / dim)
    copies[0].wait()
    normed_ref[...] = (wide * lax.rsqrt(mean + 1e-06) * gain_ref[...]).astype(BF16)
    copies[1].wait()
    main = both_ref[:, 0:rows]
    for q in range(3):
        mats = jnp.concatenate([main, both_ref[:, rows * (q + 1) : rows * (q + 2)]], axis=1)
        source = jnp.concatenate([normed_ref[:, q * third : (q + 1) * third], normed_ref[:, 3 * third :]], axis=0)
        out_ref[:, q * third : (q + 1) * third] = mm(mats, source).astype(BF16)


def shared_kernel(normed_ref, residual_ref, gate_ref, up_ref, down_ref, chosen_ref, weight_ref, out_ref, mats_ref):
    @pl.when(pl.program_id(0) == 0)
    def _():
        out_ref[...] = residual_ref[...].astype(F32)
        rows = normed_ref.shape[0]
        experts = mats_ref.shape[1] // WIDE
        chosen = chosen_ref[...]
        expert = iota((experts, rows), 0)
        weights = jnp.zeros((experts, rows), F32)
        for k in range(chosen.shape[0]):
            weights = weights + jnp.where(chosen[k : k + 1, :] == expert, weight_ref[k : k + 1, :], 0.0)
        lanes = expert_rows(experts)
        slots = mm(slot_table(chosen, experts).T.astype(BF16), lanes, ((1,), (1,)))
        spread_weights = mm(weights.T.astype(BF16), lanes, ((1,), (1,)))
        place = (iota(slots.shape, 1) % WIDE).astype(F32)
        mats_ref[0:rows, :] = jnp.where(slots == place + 1.0, spread_weights, 0.0).astype(BF16)
        for k in range(3):
            hit = (place >= 6.0) & (slots == 3.0 * place + (k - 17.0))
            mats_ref[rows * (k + 1) : rows * (k + 2), :] = jnp.where(hit, spread_weights, 0.0).astype(BF16)

    normed = normed_ref[...]
    hidden = (silu(mm(normed, gate_ref[...])) * mm(normed, up_ref[...])).astype(BF16)
    out_ref[...] += mm(hidden, down_ref[...])


def turn(value, by):
    return pltpu.roll(value, by % WIDE, axis=1)


def compact(value):
    width = value.shape[1]
    value = value.reshape(-1, 4, WIDE, width)
    row = iota((value.shape[0], WIDE, width), 1)
    a, b, c = turn(value[:, 1], 6), turn(value[:, 2], 4), turn(value[:, 3], 2)
    out = [jnp.where(row < 6, value[:, 0], a), jnp.where(row < 4, a, b), jnp.where(row < 2, b, c)]
    return jnp.concatenate(out, axis=1).reshape(-1, width)


def expand(value):
    value = value.reshape(-1, 3 * WIDE, value.shape[1])
    a, b, c = value[:, 0:WIDE], value[:, WIDE : 2 * WIDE], value[:, 2 * WIDE :]
    row = iota(a.shape, 1)
    return [a, jnp.where(row < 2, turn(a, 2), turn(b, 2)), jnp.where(row < 4, turn(b, 4), turn(c, 4)), turn(c, 6)]


def expert_kernel(x_ref, gate_ref, up_ref, down_ref, out_hbm, full_ref, out_ref, sems):
    total, wide = x_ref.shape
    third = wide // 3
    rows = out_ref.shape[1]
    row = iota((LANES // WIDE, WIDE, third), 1)
    copies = []
    for n in range(total // rows):
        for at in range(0, rows, LANES):
            dense = slice(at * SLOTS // WIDE, (at + LANES) * SLOTS // WIDE)
            tail = jnp.zeros(row.shape, F32)
            for q in range(3):
                part = x_ref[n * rows + at : n * rows + at + LANES, q * third : (q + 1) * third].astype(F32)
                full_ref[dense, q * third : (q + 1) * third] = compact(part).astype(BF16)
                part = part.reshape(row.shape)
                tail = jnp.where(row == q, turn(part, q - 6), jnp.where(row == 3 + q, turn(part, q - 4), tail))
            full_ref[dense, wide:] = compact(tail.reshape(LANES, third)).astype(BF16)
        full = full_ref[...]
        hidden = (silu(mm(full, gate_ref[...])) * mm(full, up_ref[...])).astype(BF16)
        tails = expand(mm(hidden, down_ref[:, wide:]))
        for q in range(3):
            part = slice(q * third, (q + 1) * third)
            mains = expand(mm(hidden, down_ref[:, part]))
            at = iota(mains[0].shape, 1)
            mixed = [
                jnp.where(at < 6, main, jnp.where(at == 6, turn(tail, 6 - q), turn(tail, 4 - q)))
                for main, tail in zip(mains, tails)
            ]
            out_ref[n, :, part] = jnp.stack(mixed, axis=1).reshape(rows, third).astype(BF16)
        copy = pltpu.make_async_copy(out_ref.at[n], out_hbm.at[n * rows : (n + 1) * rows, :], sems.at[n])
        copy.start()
        copies.append(copy)
    for copy in copies:
        copy.wait()


def combine_kernel(got_ref, base_hbm, mats_hbm, out_ref, base_ref, mats_ref, main_ref, sems):
    rows, dim = base_ref.shape
    third = got_ref.shape[1] // 3
    copies = fetch((
        (mats_hbm.at[0 : 2 * rows, :], mats_ref.at[0 : 2 * rows, :]), (mats_hbm.at[2 * rows :, :], mats_ref.at[2 * rows :, :]),
        (base_hbm, base_ref),
    ), sems)
    copies[0].wait()
    both = mm(mats_ref[0 : 2 * rows, :], got_ref[:, 0:third])
    main_ref[:, 0:third], tail = both[0:rows], both[rows:]
    copies[1].wait()
    for q in (1, 2):
        got = got_ref[:, q * third : (q + 1) * third]
        main_ref[:, q * third : (q + 1) * third] = mm(mats_ref[0:rows, :], got)
        tail = tail + mm(mats_ref[rows * (q + 1) : rows * (q + 2), :], got)
    copies[2].wait()
    out_ref[:, 0 : 3 * third] = (base_ref[:, 0 : 3 * third] + main_ref[...]).astype(BF16)
    out_ref[:, 3 * third :] = (base_ref[:, 3 * third :] + tail).astype(BF16)


def shape(dims, dtype=F32):
    return jax.ShapeDtypeStruct(dims, dtype)


def on_device(
    stream,
    head_input_signal,
    write_input_vectors,
    read_input_vectors,
    output_gate_input,
    step_size_input,
    position_log_decay,
    signal_filter_taps,
    write_filter_taps,
    read_filter_taps,
    step_size_bias,
    head_decay_rate,
    head_direct_term,
    grouped_norm_gain,
    mixer_output_weight,
    expert_norm_gain,
    chosen_expert_index,
    chosen_expert_weight,
    routed_gate_weight,
    routed_up_weight,
    routed_down_weight,
    common_gate_weight,
    common_up_weight,
    common_down_weight,
):
    length, chans = head_input_signal.shape
    vecs = write_input_vectors.shape[1]
    rows, dim = stream.shape
    hidden = common_gate_weight.shape[1]
    experts = lax.axis_size(SP_TP)
    wide = dim * SLOTS // WIDE

    heads = step_size_input.shape[1]
    devices = lax.axis_size(SP)
    rim = pl.pallas_call(
        rim_kernel,
        in_specs=offchip(3),
        out_specs=onchip(1)[0],
        out_shape=shape((8, chans + 2 * vecs), BF16),
        scratch_shapes=[pltpu.SemaphoreType.DMA((3,))],
        compiler_params=room(2),
        name="rim",
    )(*stay(head_input_signal, write_input_vectors, read_input_vectors))
    rim = lax.ppermute(rim, SP, [(i, i + 1) for i in range(devices - 1)])
    signal, write_rows, read_rows, cum, cum_rows, dtv, first, second, begin, taps = pl.pallas_call(
        front_kernel,
        in_specs=offchip(10),
        out_specs=tuple(onchip(10)),
        out_shape=(
            shape((length, chans)), shape((length, vecs), BF16), shape((length, vecs), BF16), shape((length, LANES)),
            shape((heads, length)), shape((length, LANES)), shape((STATE, chans)), shape((STATE, chans)),
            shape((HEAD, chans + 2 * vecs)), shape((8, chans + 2 * vecs)),
        ),
        scratch_shapes=[
            pltpu.VMEM((length, chans), BF16), pltpu.VMEM((length, vecs), BF16), pltpu.VMEM((length, vecs), BF16),
            pltpu.VMEM((heads, length), BF16), pltpu.VMEM((heads, length), F32),
            pltpu.VMEM((4, chans), BF16), pltpu.VMEM((4, vecs), BF16), pltpu.VMEM((4, vecs), BF16),
            pltpu.VMEM((1, heads), F32), pltpu.VMEM((1, heads), F32),
            pltpu.VMEM((length + 8, chans + 2 * vecs), F32), pltpu.VMEM((LANES, length), F32),
            pltpu.SemaphoreType.DMA((10,)),
        ],
        cost_estimate=pl.CostEstimate(flops=800_000_000, transcendentals=1_000_000, bytes_accessed=4_000_000),
        compiler_params=room(14),
        name="front",
    )(*stay(
        head_input_signal, write_input_vectors, read_input_vectors, step_size_input.T, position_log_decay.T,
        signal_filter_taps, write_filter_taps, read_filter_taps, step_size_bias[None], head_decay_rate[None],
    ))
    sig, wv, rv, s0, send = pl.pallas_call(
        head_kernel,
        in_specs=onchip(10),
        out_specs=tuple(onchip(5)),
        out_shape=(
            shape((length, chans)), shape((length, vecs), BF16), shape((length, vecs), BF16),
            shape((STATE, chans)), shape((STATE, chans + LANES), BF16),
        ),
        scratch_shapes=[pltpu.VMEM((HEAD + 8, chans + 2 * vecs), F32)],
        compiler_params=room(8),
        name="head",
    )(rim, begin, taps, signal, write_rows, read_rows, cum, dtv, first, second)
    in_plane = lax.axis_size(PLANE)
    got = lax.all_to_all(send, PLANE, split_axis=0, concat_axis=0, tiled=True)
    chosen = chosen_expert_index.T
    near, both = pl.pallas_call(
        near_kernel,
        in_specs=onchip(9),
        out_specs=(onchip(1)[0], offchip(1)[0]),
        out_shape=(shape((length, chans)), pltpu.HBM((experts * WIDE, 4 * rows), BF16)),
        scratch_shapes=[pltpu.VMEM((8, LANES), F32), pltpu.VMEM((experts * WIDE, 4 * rows), BF16), pltpu.SemaphoreType.DMA],
        cost_estimate=pl.CostEstimate(flops=400_000_000, transcendentals=1_000_000, bytes_accessed=4_000_000),
        compiler_params=room(18),
        name="near",
    )(sig, wv, rv, cum, cum_rows, dtv, s0, head_direct_term[None], chosen)
    planes = lax.axis_size("sp_0")
    pin, pdec, total = pl.pallas_call(
        plane_kernel,
        in_specs=onchip(1),
        out_specs=tuple(onchip(3)),
        out_shape=(shape((STATE, chans)), shape((in_plane, chans)), shape((8 * planes, chans + LANES))),
        compiler_params=room(6),
        name="plane",
    )(got)
    lower = lax.all_to_all(total, "sp_0", split_axis=0, concat_axis=0, tiled=True)
    back = pl.pallas_call(
        planes_kernel,
        in_specs=[pl.BlockSpec(memory_space=pltpu.SMEM)] + onchip(3),
        out_specs=onchip(1)[0],
        out_shape=shape((STATE, chans), BF16),
        compiler_params=room(6),
        name="planes",
    )(lax.axis_index("sp_0").astype(jnp.int32).reshape(1), pin, pdec, lower)
    incoming = lax.all_to_all(back, PLANE, split_axis=0, concat_axis=0, tiled=True)

    half = lax.axis_index("tp").astype(jnp.int32).reshape(1)
    other, mine, projection = pl.pallas_call(
        project_kernel,
        in_specs=[pl.BlockSpec(memory_space=pltpu.SMEM)] + onchip(4) + offchip(3),
        out_specs=tuple(onchip(3)),
        out_shape=(shape((rows, dim), BF16), shape((rows, chans), BF16), shape((chans, dim), BF16)),
        scratch_shapes=[
            pltpu.VMEM((length, chans), BF16), pltpu.VMEM((1, chans), F32), pltpu.VMEM((length, chans), BF16),
            pltpu.SemaphoreType.DMA((6,)),
        ],
        compiler_params=room(16),
        name="project",
    )(half, near, incoming, rv, cum, *stay(output_gate_input, grouped_norm_gain[None], mixer_output_weight))
    partner = lax.ppermute(other, "tp", [(0, 1), (1, 0)])
    own = pl.pallas_call(
        own_kernel,
        in_specs=onchip(2) + offchip(1),
        out_specs=onchip(1)[0],
        out_shape=shape((rows, dim)),
        scratch_shapes=[pltpu.VMEM((rows, dim), BF16), pltpu.SemaphoreType.DMA],
        cost_estimate=pl.CostEstimate(flops=600_000_000, transcendentals=0, bytes_accessed=6_000_000),
        compiler_params=room(10),
        name="own",
    )(mine, projection, *stay(stream))

    residual, normed, outgoing = pl.pallas_call(
        dispatch_kernel,
        in_specs=onchip(2) + offchip(2),
        out_specs=tuple(onchip(3)),
        out_shape=(shape((rows, dim), BF16), shape((rows, dim), BF16), shape((experts * WIDE, wide), BF16)),
        scratch_shapes=[pltpu.VMEM((1, dim), F32), pltpu.VMEM((experts * WIDE, 4 * rows), BF16), pltpu.SemaphoreType.DMA((2,))],
        compiler_params=room(16),
        name="dispatch",
    )(own, partner, *stay(expert_norm_gain[None], both))
    arrived = lax.all_to_all(outgoing, SP_TP, split_axis=0, concat_axis=0, tiled=True)

    part = 128
    fanout = chosen.shape[0]
    base, mats = pl.pallas_call(
        shared_kernel,
        grid=(hidden // part,),
        in_specs=[
            whole((rows, dim)), whole((rows, dim)), pl.BlockSpec((dim, part), lambda n: (0, n)),
            pl.BlockSpec((dim, part), lambda n: (0, n)), pl.BlockSpec((part, dim), lambda n: (n, 0)),
            whole((fanout, rows)), whole((fanout, rows)),
        ],
        out_specs=(whole((rows, dim)), whole((4 * rows, experts * WIDE))),
        out_shape=(pltpu.HBM((rows, dim), F32), pltpu.HBM((4 * rows, experts * WIDE), BF16)),
        cost_estimate=pl.CostEstimate(flops=800_000_000, transcendentals=70_000, bytes_accessed=8_000_000),
        compiler_params=room(16),
        name="shared",
    )(normed, residual, *stay(common_gate_weight, common_up_weight, common_down_weight), chosen, chosen_expert_weight.T)

    chunks = 2
    tall = experts * WIDE // chunks
    served = pl.pallas_call(
        expert_kernel,
        in_specs=onchip(4),
        out_specs=offchip(1)[0],
        out_shape=pltpu.HBM((experts * WIDE, wide), BF16),
        scratch_shapes=[pltpu.VMEM((tall * SLOTS // WIDE, dim), BF16), pltpu.VMEM((chunks, tall, wide), BF16), pltpu.SemaphoreType.DMA((chunks,))],
        compiler_params=room(24),
        name="experts",
    )(arrived, routed_gate_weight[0], routed_up_weight[0], routed_down_weight[0])
    returned = lax.all_to_all(served, SP_TP, split_axis=0, concat_axis=0, tiled=True)

    return pl.pallas_call(
        combine_kernel,
        in_specs=onchip(1) + offchip(2),
        out_specs=onchip(1)[0],
        out_shape=shape((rows, dim), BF16),
        scratch_shapes=[pltpu.VMEM((rows, dim), F32), pltpu.VMEM((4 * rows, experts * WIDE), BF16), pltpu.VMEM((rows, wide), F32), pltpu.SemaphoreType.DMA((3,))],
        compiler_params=room(16),
        name="combine",
    )(returned, *stay(base, mats))


def solution(mesh):
    split = Mesh(mesh.devices.reshape(4, 4, 4, mesh.shape["tp"]), ("sp_0", "sp_1", "sp_2", "tp"))
    return jax.shard_map(
        on_device,
        mesh=split,
        in_specs=(
            P(SP_TP, None),
            P(SP, "tp"),
            P(SP, "tp"),
            P(SP, "tp"),
            P(SP, "tp"),
            P(SP, "tp"),
            P(SP, "tp"),
            P(None, "tp"),
            P(None, "tp"),
            P(None, "tp"),
            P("tp"),
            P("tp"),
            P("tp"),
            P("tp"),
            P("tp", None),
            P(),
            P(SP_TP, None),
            P(SP_TP, None),
            P(SP_TP, None, None),
            P(SP_TP, None, None),
            P(SP_TP, None, None),
            P(),
            P(),
            P(),
        ),
        out_specs=P(SP_TP, None),
        check_vma=False,
    )
```

```python
import jax
import jax.numpy as jnp
from jax import lax
from jax.experimental import pallas as pl
from jax.experimental.pallas import tpu as pltpu
from jax.sharding import Mesh
from jax.sharding import PartitionSpec as P

HEAD_DIM = 64
STATE = 128
BLK = 128
HEAD = 16
LANES = 128
SLOTS = 6
WIDE = 8
SP = ("sp_0", "sp_1", "sp_2")
PLANE = ("sp_1", "sp_2")
SP_TP = ("sp_0", "sp_1", "sp_2", "tp")
F32 = jnp.float32
BF16 = jnp.bfloat16


def mm(a, b, dims=((1,), (0,)), precision=None):
    return lax.dot_general(a, b, (dims, ((), ())), precision=precision, preferred_element_type=F32)


def iota(shape, dim):
    return lax.broadcasted_iota(jnp.int32, shape, dim)


def head_lanes(width):
    return jnp.where(iota((LANES, width), 1) // HEAD_DIM == iota((LANES, width), 0), 1.0, 0.0).astype(BF16)


def spread(values, lanes):
    high = values.astype(BF16)
    low = (values - high.astype(F32)).astype(BF16)
    return mm(high, lanes) + mm(low, lanes)


def silu(v):
    return v * (1.0 / (1.0 + jnp.exp(-v)))


def onchip(count):
    return [pl.BlockSpec(memory_space=pltpu.VMEM)] * count


def offchip(count):
    return [pl.BlockSpec(memory_space=pltpu.HBM)] * count


def stay(*arrays):
    return [pltpu.with_memory_space_constraint(array, pltpu.HBM) for array in arrays]


def room(mebibytes):
    return pltpu.CompilerParams(vmem_limit_bytes=mebibytes << 20)


def whole(shape):
    return pl.BlockSpec(shape, lambda *_: (0,) * len(shape))


def fetch(pairs, sems):
    copies = [pltpu.make_async_copy(src, dst, sems.at[i]) for i, (src, dst) in enumerate(pairs)]
    for copy in copies:
        copy.start()
    return copies


def rim_kernel(x_ref, b_ref, c_ref, out_ref, sems):
    start, pairs = 0, []
    for ref in (x_ref, b_ref, c_ref):
        rows, size = ref.shape
        pairs.append((ref.at[rows - 8 : rows, :], out_ref.at[:, start : start + size]))
        start += size
    for copy in fetch(pairs, sems):
        copy.wait()


def filtered(ext_ref, taps, lanes, first, count):
    total = taps[0:1] * ext_ref[first : first + count, lanes]
    for k in range(1, 4):
        total = total + taps[k : k + 1] * ext_ref[first + k : first + k + count, lanes]
    return silu(total)


def front_kernel(x_hbm, b_hbm, c_hbm, dt_hbm, pld_hbm, tx_hbm, tb_hbm, tc_hbm, bias_hbm, rate_hbm,
                 sig_ref, wv_ref, rv_ref, cum_ref, rows_ref, dtv_ref, s0_ref, s1_ref, begin_ref, taps_ref,
                 x_ref, b_ref, c_ref, dt_ref, pld_ref, tx_ref, tb_ref, tc_ref, bias_ref, rate_ref, ext_ref, wide_ref, sems):
    length, chans = x_ref.shape
    vecs = b_ref.shape[1]
    heads = dt_ref.shape[0]
    groups = vecs // STATE
    width = chans // groups
    copies = fetch((
        (bias_hbm, bias_ref), (rate_hbm, rate_ref), (dt_hbm, dt_ref), (pld_hbm, pld_ref), (tx_hbm, tx_ref), (tb_hbm, tb_ref),
        (tc_hbm, tc_ref), (b_hbm, b_ref), (c_hbm, c_ref), (x_hbm, x_ref),
    ), sems)
    for copy in copies[0:4]:
        copy.wait()
    wide_ref[...] = jnp.zeros_like(wide_ref)
    wide_ref[0:1, 0:heads] = bias_ref[...]
    wide_ref[1:2, 0:heads] = rate_ref[...]
    columns = wide_ref[:, 0:LANES].T
    v = dt_ref[...].astype(F32) + columns[0:heads, 0:1]
    step = jnp.maximum(v, 0.0) + jnp.log(1.0 + jnp.exp(-jnp.abs(v)))
    logs = pld_ref[...] - columns[0:heads, 1:2] * step
    upper = jnp.where(iota((length, length), 0) <= iota((length, length), 1), 1.0, 0.0)
    sums = mm(logs, upper, precision=lax.Precision.HIGHEST)
    rows_ref[...] = sums
    wide_ref[0:heads, :] = step
    dtv_ref[...] = wide_ref[...].T
    wide_ref[0:heads, :] = sums
    cum = wide_ref[...].T
    cum_ref[...] = cum
    half_end, end = cum[BLK - 1 : BLK], cum[length - 1 : length]
    ends = jnp.where(iota((length, LANES), 0) < BLK, half_end, end)
    weights = jnp.where(iota((length, LANES), 0) < HEAD, 0.0, dtv_ref[...] * jnp.exp(ends - cum))
    scale = spread(weights, head_lanes(chans))
    for copy in copies[4:7]:
        copy.wait()
    taps_ref[...] = jnp.zeros_like(taps_ref)
    sources = (
        (b_ref, tb_ref, chans, vecs, wv_ref, copies[7]), (c_ref, tc_ref, chans + vecs, vecs, rv_ref, copies[8]),
        (x_ref, tx_ref, 0, chans, sig_ref, copies[9]),
    )
    ext_ref[0:8, :] = jnp.zeros((8, ext_ref.shape[1]), F32)
    for src, taps, start, size, dst, copy in sources:
        taps_ref[0:4, start : start + size] = taps[...].astype(F32)
        copy.wait()
        ext_ref[8 : 8 + length, start : start + size] = src[...].astype(F32)
        begin_ref[:, start : start + size] = src[0:HEAD, :].astype(F32)
        for at in range(0, size, 256):
            lanes = slice(start + at, start + at + 256)
            dst[:, at : at + 256] = filtered(ext_ref, taps_ref[:, lanes], lanes, 5, length).astype(dst.dtype)
    for g in range(groups):
        part = slice(g * width, (g + 1) * width)
        vec = slice(g * STATE, (g + 1) * STATE)
        scaled = (sig_ref[:, part] * scale[:, part]).astype(BF16)
        s0_ref[:, part] = mm(wv_ref[0:BLK, vec], scaled[0:BLK], ((0,), (0,)))
        s1_ref[:, part] = mm(wv_ref[BLK:length, vec], scaled[BLK:length], ((0,), (0,)))


def head_kernel(rim_ref, begin_ref, taps_ref, siga_ref, wva_ref, rva_ref, cum_ref, dtv_ref, s0a_ref, s1_ref,
                sig_ref, wv_ref, rv_ref, s0_ref, send_ref, ext_ref):
    length, chans = siga_ref.shape
    vecs = wva_ref.shape[1]
    groups = vecs // STATE
    width = chans // groups
    ext_ref[0:8, :] = rim_ref[...].astype(F32)
    ext_ref[8 : 8 + HEAD, :] = begin_ref[...]
    for start, size, old, new in ((0, chans, siga_ref, sig_ref), (chans, vecs, wva_ref, wv_ref), (chans + vecs, vecs, rva_ref, rv_ref)):
        lanes = slice(start, start + size)
        new[0:HEAD, :] = filtered(ext_ref, taps_ref[:, lanes], lanes, 5, HEAD).astype(new.dtype)
        new[HEAD:, :] = old[HEAD:, :]
    half_end, end = cum_ref[BLK - 1 : BLK, :], cum_ref[length - 1 : length, :]
    lanes = head_lanes(chans)
    scale = spread(dtv_ref[0:HEAD, :] * jnp.exp(half_end - cum_ref[0:HEAD, :]), lanes)
    passing = spread(jnp.broadcast_to(jnp.exp(end - half_end), (8, LANES)), lanes)[0:1]
    scaled = (sig_ref[0:HEAD, :] * scale).astype(BF16)
    for g in range(groups):
        part = slice(g * width, (g + 1) * width)
        first = s0a_ref[:, part] + mm(wv_ref[0:HEAD, g * STATE : (g + 1) * STATE], scaled[:, part], ((0,), (0,)))
        s0_ref[:, part] = first
        send_ref[:, part] = (first * passing[:, part] + s1_ref[:, part]).astype(BF16)
    high = end.astype(BF16).astype(F32)
    mid = (end - high).astype(BF16).astype(F32)
    low = (end - high - mid).astype(BF16).astype(F32)
    row = iota((STATE, LANES), 0) % 8
    send_ref[:, chans : chans + LANES] = jnp.where(
        row == 0, high, jnp.where(row == 1, mid, jnp.where(row == 2, low, 0.0))
    ).astype(BF16)


def plane_kernel(got_ref, pin_ref, pdec_ref, send_ref):
    count = got_ref.shape[0] // 8
    chans = got_ref.shape[1] - LANES
    logs = jnp.sum(got_ref[:, chans:].astype(F32).reshape(count, 8, LANES), axis=1)
    lanes = head_lanes(chans)
    decay = spread(jnp.exp(logs), lanes)
    state = jnp.zeros((8, chans), F32)
    sofar = jnp.zeros((1, LANES), F32)
    before = []
    for i in range(count):
        pin_ref[8 * i : 8 * i + 8, :] = state
        before.append(sofar)
        state = state * decay[i : i + 1] + got_ref[8 * i : 8 * i + 8, 0:chans].astype(F32)
        sofar = sofar + logs[i : i + 1]
    pdec_ref[...] = spread(jnp.exp(jnp.concatenate(before, axis=0)), lanes)
    for k in range(send_ref.shape[0] // 8):
        send_ref[8 * k : 8 * k + 8, 0:chans] = state
        send_ref[8 * k : 8 * k + 8, chans:] = jnp.broadcast_to(sofar, (8, LANES))


def planes_kernel(plane_ref, pin_ref, pdec_ref, got_ref, out_ref):
    chans = pin_ref.shape[1]
    count = pin_ref.shape[0] // 8
    lanes = head_lanes(chans)
    plane = plane_ref[0]
    state = jnp.zeros((8, chans), F32)
    for k in range(got_ref.shape[0] // 8 - 1):
        rows = slice(8 * k, 8 * k + 8)
        state = jnp.where(k < plane, state * spread(jnp.exp(got_ref[rows, chans:]), lanes) + got_ref[rows, 0:chans], state)
    for i in range(0, count, 2):
        pair = [pin_ref[8 * k : 8 * k + 8, :] + state * pdec_ref[k : k + 1, :] for k in (i, i + 1)]
        out_ref[8 * i : 8 * i + 16, :] = jnp.concatenate(pair, axis=0).astype(BF16)


def near_kernel(sig_ref, wv_ref, rv_ref, cum_ref, rows_ref, dtv_ref, s0_ref, direct_ref, chosen_ref, y_ref, both_hbm, pad_ref, both_ref, sem):
    experts, tokens = both_ref.shape[0] // WIDE, chosen_ref.shape[1]
    slots = mm(expert_rows(experts), slot_table(chosen_ref[...], experts).astype(BF16))
    place = (iota(slots.shape, 0) % WIDE).astype(F32)
    both_ref[:, 0:tokens] = jnp.where(slots == place + 1.0, 1.0, 0.0).astype(BF16)
    for q in range(3):
        tail = jnp.where((place >= 6.0) & (slots == 3.0 * place + (q - 17.0)), 1.0, 0.0)
        both_ref[:, tokens * (q + 1) : tokens * (q + 2)] = tail.astype(BF16)
    copy = pltpu.make_async_copy(both_ref, both_hbm, sem)
    copy.start()
    length, chans = sig_ref.shape
    heads = direct_ref.shape[1]
    groups = wv_ref.shape[1] // STATE
    width = chans // groups
    lanes = head_lanes(chans)
    cum = cum_ref[...]
    cum_rows = rows_ref[...]
    pad_ref[...] = jnp.zeros_like(pad_ref)
    pad_ref[:, 0:heads] = jnp.broadcast_to(direct_ref[...], (8, heads))
    direct = spread(pad_ref[...], lanes)[0:1]
    scaled = (sig_ref[...] * spread(dtv_ref[...], lanes)).astype(BF16)
    causal = iota((BLK, BLK), 0) >= iota((BLK, BLK), 1)
    left = iota((BLK, LANES), 1) < HEAD_DIM
    into = spread(jnp.exp(cum[BLK:length] - cum[BLK - 1 : BLK]), lanes)
    for b in range(length // BLK):
        rows = slice(b * BLK, (b + 1) * BLK)
        for g in range(groups):
            vec = slice(g * STATE, (g + 1) * STATE)
            part = slice(g * width, (g + 1) * width)
            products = mm(rv_ref[rows, vec], wv_ref[rows, vec], ((1,), (1,)))
            if b == 1:
                carried = mm(rv_ref[rows, vec], s0_ref[:, part].astype(BF16)) * into[:, part]
            for j in range(width // LANES):
                at = g * width + j * LANES
                mats = []
                for h in (at // HEAD_DIM, at // HEAD_DIM + 1):
                    gap = cum[rows, h : h + 1] - cum_rows[h : h + 1, rows]
                    mats.append((products * jnp.exp(jnp.where(causal, gap, -1e30))).astype(BF16))
                pair = scaled[rows, at : at + LANES]
                zero = jnp.zeros_like(pair)
                stacked = jnp.concatenate([jnp.where(left, pair, zero), jnp.where(left, zero, pair)], axis=0)
                out = mm(jnp.concatenate(mats, axis=1), stacked)
                out = out + direct[:, at : at + LANES] * sig_ref[rows, at : at + LANES]
                if b == 1:
                    out = out + carried[:, j * LANES : (j + 1) * LANES]
                y_ref[rows, at : at + LANES] = out
    copy.wait()


def project_kernel(half_ref, y_ref, state_ref, rv_ref, cum_ref, gate_hbm, gain_hbm, w_hbm, other_ref, mine_ref, w_ref,
                   gate_ref, gain_ref, mix_ref, sems):
    length, chans = y_ref.shape
    groups = rv_ref.shape[1] // STATE
    width = chans // groups
    rows, dim = other_ref.shape
    parts = 4
    pairs = [(gate_hbm, gate_ref), (gain_hbm, gain_ref)]
    for k in range(parts):
        part = pl.ds(k * (dim // parts), dim // parts)
        pairs.append((w_hbm.at[:, part], w_ref.at[:, part]))
    copies = fetch(pairs, sems)
    scale = spread(jnp.exp(cum_ref[...]), head_lanes(chans))
    for g in range(groups):
        part = slice(g * width, (g + 1) * width)
        far = mm(rv_ref[:, g * STATE : (g + 1) * STATE], state_ref[:, part])
        inner = y_ref[:, part] + far * scale[:, part]
        if g == 0:
            copies[0].wait()
            copies[1].wait()
        gated = inner * silu(gate_ref[:, part].astype(F32))
        mean = jnp.sum(gated * gated, axis=1, keepdims=True) * (1.0 / width)
        mix_ref[:, part] = (gated * lax.rsqrt(mean + 1e-06) * gain_ref[:, part]).astype(BF16)
    half = half_ref[0]
    mine_ref[...] = mix_ref[pl.ds(pl.multiple_of(half * rows, rows), rows), :]
    theirs = mix_ref[pl.ds(pl.multiple_of((1 - half) * rows, rows), rows), :]
    for k in range(parts):
        part = slice(k * (dim // parts), (k + 1) * (dim // parts))
        copies[2 + k].wait()
        other_ref[:, part] = mm(theirs, w_ref[:, part]).astype(BF16)


def own_kernel(mine_ref, w_ref, stream_hbm, both_hbm, gain_hbm, own_ref, both_ref, gain_ref, stream_ref, sems):
    copies = fetch(((stream_hbm, stream_ref), (both_hbm, both_ref), (gain_hbm, gain_ref)), sems)
    product = mm(mine_ref[...], w_ref[...])
    copies[0].wait()
    own_ref[...] = product + stream_ref[...].astype(F32)
    for copy in copies[1:]:
        copy.wait()


def slot_table(chosen, experts):
    count = chosen.shape[1]
    expert = iota((experts, count), 0)
    named = jnp.zeros((experts, count), F32)
    for k in range(chosen.shape[0]):
        named = named + jnp.where(chosen[k : k + 1, :] == expert, 1.0, 0.0)
    earlier = jnp.where(iota((count, count), 0) < iota((count, count), 1), 1.0, 0.0).astype(BF16)
    return named * (mm(named.astype(BF16), earlier) + 1.0)


def expert_rows(experts):
    return jnp.where(iota((experts * WIDE, experts), 0) // WIDE == iota((experts * WIDE, experts), 1), 1.0, 0.0).astype(BF16)


def dispatch_kernel(own_ref, got_ref, both_ref, gain_ref, residual_ref, normed_ref, out_ref):
    rows, dim = own_ref.shape
    third = out_ref.shape[1] // 3
    residual = (own_ref[...] + got_ref[...].astype(F32)).astype(BF16)
    residual_ref[...] = residual
    wide = residual.astype(F32)
    mean = jnp.sum(wide * wide, axis=1, keepdims=True) * (1.0 / dim)
    normed_ref[...] = (wide * lax.rsqrt(mean + 1e-06) * gain_ref[...]).astype(BF16)
    main = both_ref[:, 0:rows]
    for q in range(3):
        mats = jnp.concatenate([main, both_ref[:, rows * (q + 1) : rows * (q + 2)]], axis=1)
        source = jnp.concatenate([normed_ref[:, q * third : (q + 1) * third], normed_ref[:, 3 * third :]], axis=0)
        out_ref[:, q * third : (q + 1) * third] = mm(mats, source).astype(BF16)


def shared_kernel(normed_ref, residual_ref, gate_ref, up_ref, down_ref, chosen_ref, weight_ref, out_ref, mats_ref):
    @pl.when(pl.program_id(0) == 0)
    def _():
        out_ref[...] = residual_ref[...].astype(F32)
        rows = normed_ref.shape[0]
        experts = mats_ref.shape[1] // WIDE
        chosen = chosen_ref[...]
        expert = iota((experts, rows), 0)
        weights = jnp.zeros((experts, rows), F32)
        for k in range(chosen.shape[0]):
            weights = weights + jnp.where(chosen[k : k + 1, :] == expert, weight_ref[k : k + 1, :], 0.0)
        lanes = expert_rows(experts)
        slots = mm(slot_table(chosen, experts).T.astype(BF16), lanes, ((1,), (1,)))
        spread_weights = mm(weights.T.astype(BF16), lanes, ((1,), (1,)))
        place = (iota(slots.shape, 1) % WIDE).astype(F32)
        mats_ref[0:rows, :] = jnp.where(slots == place + 1.0, spread_weights, 0.0).astype(BF16)
        for k in range(3):
            hit = (place >= 6.0) & (slots == 3.0 * place + (k - 17.0))
            mats_ref[rows * (k + 1) : rows * (k + 2), :] = jnp.where(hit, spread_weights, 0.0).astype(BF16)

    normed = normed_ref[...]
    hidden = (silu(mm(normed, gate_ref[...])) * mm(normed, up_ref[...])).astype(BF16)
    out_ref[...] += mm(hidden, down_ref[...])


def turn(value, by):
    return pltpu.roll(value, by % WIDE, axis=1)


def compact(value):
    width = value.shape[1]
    value = value.reshape(-1, 4, WIDE, width)
    row = iota((value.shape[0], WIDE, width), 1)
    a, b, c = turn(value[:, 1], 6), turn(value[:, 2], 4), turn(value[:, 3], 2)
    out = [jnp.where(row < 6, value[:, 0], a), jnp.where(row < 4, a, b), jnp.where(row < 2, b, c)]
    return jnp.concatenate(out, axis=1).reshape(-1, width)


def expand(value):
    value = value.reshape(-1, 3 * WIDE, value.shape[1])
    a, b, c = value[:, 0:WIDE], value[:, WIDE : 2 * WIDE], value[:, 2 * WIDE :]
    row = iota(a.shape, 1)
    return [a, jnp.where(row < 2, turn(a, 2), turn(b, 2)), jnp.where(row < 4, turn(b, 4), turn(c, 4)), turn(c, 6)]


def expert_kernel(x_ref, gate_ref, up_ref, down_ref, out_hbm, full_ref, out_ref, sems):
    total, wide = x_ref.shape
    third = wide // 3
    rows = out_ref.shape[1]
    row = iota((LANES // WIDE, WIDE, third), 1)
    copies = []
    for n in range(total // rows):
        for at in range(0, rows, LANES):
            dense = slice(at * SLOTS // WIDE, (at + LANES) * SLOTS // WIDE)
            tail = jnp.zeros(row.shape, F32)
            for q in range(3):
                part = x_ref[n * rows + at : n * rows + at + LANES, q * third : (q + 1) * third].astype(F32)
                full_ref[dense, q * third : (q + 1) * third] = compact(part).astype(BF16)
                part = part.reshape(row.shape)
                tail = jnp.where(row == q, turn(part, q - 6), jnp.where(row == 3 + q, turn(part, q - 4), tail))
            full_ref[dense, wide:] = compact(tail.reshape(LANES, third)).astype(BF16)
        full = full_ref[...]
        hidden = (silu(mm(full, gate_ref[...])) * mm(full, up_ref[...])).astype(BF16)
        tails = expand(mm(hidden, down_ref[:, wide:]))
        for q in range(3):
            part = slice(q * third, (q + 1) * third)
            mains = expand(mm(hidden, down_ref[:, part]))
            at = iota(mains[0].shape, 1)
            mixed = [
                jnp.where(at < 6, main, jnp.where(at == 6, turn(tail, 6 - q), turn(tail, 4 - q)))
                for main, tail in zip(mains, tails)
            ]
            out_ref[n, :, part] = jnp.stack(mixed, axis=1).reshape(rows, third).astype(BF16)
        copy = pltpu.make_async_copy(out_ref.at[n], out_hbm.at[n * rows : (n + 1) * rows, :], sems.at[n])
        copy.start()
        copies.append(copy)
    for copy in copies:
        copy.wait()


def combine_kernel(got_ref, base_hbm, mats_hbm, out_ref, base_ref, mats_ref, main_ref, sems):
    rows, dim = base_ref.shape
    third = got_ref.shape[1] // 3
    copies = fetch((
        (mats_hbm.at[0 : 2 * rows, :], mats_ref.at[0 : 2 * rows, :]), (mats_hbm.at[2 * rows :, :], mats_ref.at[2 * rows :, :]),
        (base_hbm, base_ref),
    ), sems)
    copies[0].wait()
    both = mm(mats_ref[0 : 2 * rows, :], got_ref[:, 0:third])
    main_ref[:, 0:third], tail = both[0:rows], both[rows:]
    copies[1].wait()
    for q in (1, 2):
        got = got_ref[:, q * third : (q + 1) * third]
        main_ref[:, q * third : (q + 1) * third] = mm(mats_ref[0:rows, :], got)
        tail = tail + mm(mats_ref[rows * (q + 1) : rows * (q + 2), :], got)
    copies[2].wait()
    out_ref[:, 0 : 3 * third] = (base_ref[:, 0 : 3 * third] + main_ref[...]).astype(BF16)
    out_ref[:, 3 * third :] = (base_ref[:, 3 * third :] + tail).astype(BF16)


def shape(dims, dtype=F32):
    return jax.ShapeDtypeStruct(dims, dtype)


def on_device(
    stream,
    head_input_signal,
    write_input_vectors,
    read_input_vectors,
    output_gate_input,
    step_size_input,
    position_log_decay,
    signal_filter_taps,
    write_filter_taps,
    read_filter_taps,
    step_size_bias,
    head_decay_rate,
    head_direct_term,
    grouped_norm_gain,
    mixer_output_weight,
    expert_norm_gain,
    chosen_expert_index,
    chosen_expert_weight,
    routed_gate_weight,
    routed_up_weight,
    routed_down_weight,
    common_gate_weight,
    common_up_weight,
    common_down_weight,
):
    length, chans = head_input_signal.shape
    vecs = write_input_vectors.shape[1]
    rows, dim = stream.shape
    hidden = common_gate_weight.shape[1]
    experts = lax.axis_size(SP_TP)
    wide = dim * SLOTS // WIDE

    heads = step_size_input.shape[1]
    devices = lax.axis_size(SP)
    rim = pl.pallas_call(
        rim_kernel,
        in_specs=offchip(3),
        out_specs=onchip(1)[0],
        out_shape=shape((8, chans + 2 * vecs), BF16),
        scratch_shapes=[pltpu.SemaphoreType.DMA((3,))],
        compiler_params=room(2),
        name="rim",
    )(*stay(head_input_signal, write_input_vectors, read_input_vectors))
    rim = lax.ppermute(rim, SP, [(i, i + 1) for i in range(devices - 1)])
    signal, write_rows, read_rows, cum, cum_rows, dtv, first, second, begin, taps = pl.pallas_call(
        front_kernel,
        in_specs=offchip(10),
        out_specs=tuple(onchip(10)),
        out_shape=(
            shape((length, chans)), shape((length, vecs), BF16), shape((length, vecs), BF16), shape((length, LANES)),
            shape((heads, length)), shape((length, LANES)), shape((STATE, chans)), shape((STATE, chans)),
            shape((HEAD, chans + 2 * vecs)), shape((8, chans + 2 * vecs)),
        ),
        scratch_shapes=[
            pltpu.VMEM((length, chans), BF16), pltpu.VMEM((length, vecs), BF16), pltpu.VMEM((length, vecs), BF16),
            pltpu.VMEM((heads, length), BF16), pltpu.VMEM((heads, length), F32),
            pltpu.VMEM((4, chans), BF16), pltpu.VMEM((4, vecs), BF16), pltpu.VMEM((4, vecs), BF16),
            pltpu.VMEM((1, heads), F32), pltpu.VMEM((1, heads), F32),
            pltpu.VMEM((length + 8, chans + 2 * vecs), F32), pltpu.VMEM((LANES, length), F32),
            pltpu.SemaphoreType.DMA((10,)),
        ],
        cost_estimate=pl.CostEstimate(flops=800_000_000, transcendentals=1_000_000, bytes_accessed=4_000_000),
        compiler_params=room(14),
        name="front",
    )(*stay(
        head_input_signal, write_input_vectors, read_input_vectors, step_size_input.T, position_log_decay.T,
        signal_filter_taps, write_filter_taps, read_filter_taps, step_size_bias[None], head_decay_rate[None],
    ))
    sig, wv, rv, s0, send = pl.pallas_call(
        head_kernel,
        in_specs=onchip(10),
        out_specs=tuple(onchip(5)),
        out_shape=(
            shape((length, chans)), shape((length, vecs), BF16), shape((length, vecs), BF16),
            shape((STATE, chans)), shape((STATE, chans + LANES), BF16),
        ),
        scratch_shapes=[pltpu.VMEM((HEAD + 8, chans + 2 * vecs), F32)],
        compiler_params=room(8),
        name="head",
    )(rim, begin, taps, signal, write_rows, read_rows, cum, dtv, first, second)
    in_plane = lax.axis_size(PLANE)
    got = lax.all_to_all(send, PLANE, split_axis=0, concat_axis=0, tiled=True)
    chosen = chosen_expert_index.T
    near, both = pl.pallas_call(
        near_kernel,
        in_specs=onchip(9),
        out_specs=(onchip(1)[0], offchip(1)[0]),
        out_shape=(shape((length, chans)), pltpu.HBM((experts * WIDE, 4 * rows), BF16)),
        scratch_shapes=[pltpu.VMEM((8, LANES), F32), pltpu.VMEM((experts * WIDE, 4 * rows), BF16), pltpu.SemaphoreType.DMA],
        cost_estimate=pl.CostEstimate(flops=400_000_000, transcendentals=1_000_000, bytes_accessed=4_000_000),
        compiler_params=room(18),
        name="near",
    )(sig, wv, rv, cum, cum_rows, dtv, s0, head_direct_term[None], chosen)
    planes = lax.axis_size("sp_0")
    pin, pdec, total = pl.pallas_call(
        plane_kernel,
        in_specs=onchip(1),
        out_specs=tuple(onchip(3)),
        out_shape=(shape((STATE, chans)), shape((in_plane, chans)), shape((8 * planes, chans + LANES))),
        compiler_params=room(6),
        name="plane",
    )(got)
    lower = lax.all_to_all(total, "sp_0", split_axis=0, concat_axis=0, tiled=True)
    back = pl.pallas_call(
        planes_kernel,
        in_specs=[pl.BlockSpec(memory_space=pltpu.SMEM)] + onchip(3),
        out_specs=onchip(1)[0],
        out_shape=shape((STATE, chans), BF16),
        compiler_params=room(6),
        name="planes",
    )(lax.axis_index("sp_0").astype(jnp.int32).reshape(1), pin, pdec, lower)
    incoming = lax.all_to_all(back, PLANE, split_axis=0, concat_axis=0, tiled=True)

    half = lax.axis_index("tp").astype(jnp.int32).reshape(1)
    other, mine, projection = pl.pallas_call(
        project_kernel,
        in_specs=[pl.BlockSpec(memory_space=pltpu.SMEM)] + onchip(4) + offchip(3),
        out_specs=tuple(onchip(3)),
        out_shape=(shape((rows, dim), BF16), shape((rows, chans), BF16), shape((chans, dim), BF16)),
        scratch_shapes=[
            pltpu.VMEM((length, chans), BF16), pltpu.VMEM((1, chans), F32), pltpu.VMEM((length, chans), BF16),
            pltpu.SemaphoreType.DMA((6,)),
        ],
        compiler_params=room(16),
        name="project",
    )(half, near, incoming, rv, cum, *stay(output_gate_input, grouped_norm_gain[None], mixer_output_weight))
    partner = lax.ppermute(other, "tp", [(0, 1), (1, 0)])
    own, both, gain = pl.pallas_call(
        own_kernel,
        in_specs=onchip(2) + offchip(3),
        out_specs=tuple(onchip(3)),
        out_shape=(shape((rows, dim)), shape((experts * WIDE, 4 * rows), BF16), shape((1, dim))),
        scratch_shapes=[pltpu.VMEM((rows, dim), BF16), pltpu.SemaphoreType.DMA((3,))],
        cost_estimate=pl.CostEstimate(flops=600_000_000, transcendentals=0, bytes_accessed=6_000_000),
        compiler_params=room(10),
        name="own",
    )(mine, projection, *stay(stream, both, expert_norm_gain[None]))

    residual, normed, outgoing = pl.pallas_call(
        dispatch_kernel,
        in_specs=onchip(4),
        out_specs=tuple(onchip(3)),
        out_shape=(shape((rows, dim), BF16), shape((rows, dim), BF16), shape((experts * WIDE, wide), BF16)),
        compiler_params=room(12),
        name="dispatch",
    )(own, partner, both, gain)
    arrived = lax.all_to_all(outgoing, SP_TP, split_axis=0, concat_axis=0, tiled=True)

    part = 128
    fanout = chosen.shape[0]
    base, mats = pl.pallas_call(
        shared_kernel,
        grid=(hidden // part,),
        in_specs=[
            whole((rows, dim)), whole((rows, dim)), pl.BlockSpec((dim, part), lambda n: (0, n)),
            pl.BlockSpec((dim, part), lambda n: (0, n)), pl.BlockSpec((part, dim), lambda n: (n, 0)),
            whole((fanout, rows)), whole((fanout, rows)),
        ],
        out_specs=(whole((rows, dim)), whole((4 * rows, experts * WIDE))),
        out_shape=(pltpu.HBM((rows, dim), F32), pltpu.HBM((4 * rows, experts * WIDE), BF16)),
        cost_estimate=pl.CostEstimate(flops=800_000_000, transcendentals=70_000, bytes_accessed=8_000_000),
        compiler_params=room(16),
        name="shared",
    )(normed, residual, *stay(common_gate_weight, common_up_weight, common_down_weight), chosen, chosen_expert_weight.T)

    chunks = 2
    tall = experts * WIDE // chunks
    served = pl.pallas_call(
        expert_kernel,
        in_specs=onchip(4),
        out_specs=offchip(1)[0],
        out_shape=pltpu.HBM((experts * WIDE, wide), BF16),
        scratch_shapes=[pltpu.VMEM((tall * SLOTS // WIDE, dim), BF16), pltpu.VMEM((chunks, tall, wide), BF16), pltpu.SemaphoreType.DMA((chunks,))],
        compiler_params=room(24),
        name="experts",
    )(arrived, routed_gate_weight[0], routed_up_weight[0], routed_down_weight[0])
    returned = lax.all_to_all(served, SP_TP, split_axis=0, concat_axis=0, tiled=True)

    return pl.pallas_call(
        combine_kernel,
        in_specs=onchip(1) + offchip(2),
        out_specs=onchip(1)[0],
        out_shape=shape((rows, dim), BF16),
        scratch_shapes=[pltpu.VMEM((rows, dim), F32), pltpu.VMEM((4 * rows, experts * WIDE), BF16), pltpu.VMEM((rows, wide), F32), pltpu.SemaphoreType.DMA((3,))],
        compiler_params=room(16),
        name="combine",
    )(returned, *stay(base, mats))


def solution(mesh):
    split = Mesh(mesh.devices.reshape(4, 4, 4, mesh.shape["tp"]), ("sp_0", "sp_1", "sp_2", "tp"))
    return jax.shard_map(
        on_device,
        mesh=split,
        in_specs=(
            P(SP_TP, None),
            P(SP, "tp"),
            P(SP, "tp"),
            P(SP, "tp"),
            P(SP, "tp"),
            P(SP, "tp"),
            P(SP, "tp"),
            P(None, "tp"),
            P(None, "tp"),
            P(None, "tp"),
            P("tp"),
            P("tp"),
            P("tp"),
            P("tp"),
            P("tp", None),
            P(),
            P(SP_TP, None),
            P(SP_TP, None),
            P(SP_TP, None, None),
            P(SP_TP, None, None),
            P(SP_TP, None, None),
            P(),
            P(),
            P(),
        ),
        out_specs=P(SP_TP, None),
        check_vma=False,
    )
```

```python
import jax
import jax.numpy as jnp
from jax import lax
from jax.experimental import pallas as pl
from jax.experimental.pallas import tpu as pltpu
from jax.sharding import Mesh
from jax.sharding import PartitionSpec as P

HEAD_DIM = 64
STATE = 128
BLK = 128
HEAD = 16
LANES = 128
SLOTS = 6
WIDE = 8
SP = ("sp_0", "sp_1", "sp_2")
PLANE = ("sp_1", "sp_2")
SP_TP = ("sp_0", "sp_1", "sp_2", "tp")
F32 = jnp.float32
BF16 = jnp.bfloat16


def mm(a, b, dims=((1,), (0,)), precision=None):
    return lax.dot_general(a, b, (dims, ((), ())), precision=precision, preferred_element_type=F32)


def iota(shape, dim):
    return lax.broadcasted_iota(jnp.int32, shape, dim)


def head_lanes(width):
    return jnp.where(iota((LANES, width), 1) // HEAD_DIM == iota((LANES, width), 0), 1.0, 0.0).astype(BF16)


def spread(values, lanes):
    high = values.astype(BF16)
    low = (values - high.astype(F32)).astype(BF16)
    return mm(high, lanes) + mm(low, lanes)


def silu(v):
    return v * (1.0 / (1.0 + jnp.exp(-v)))


def onchip(count):
    return [pl.BlockSpec(memory_space=pltpu.VMEM)] * count


def offchip(count):
    return [pl.BlockSpec(memory_space=pltpu.HBM)] * count


def stay(*arrays):
    return [pltpu.with_memory_space_constraint(array, pltpu.HBM) for array in arrays]


def room(mebibytes):
    return pltpu.CompilerParams(vmem_limit_bytes=mebibytes << 20)


def whole(shape):
    return pl.BlockSpec(shape, lambda *_: (0,) * len(shape))


def fetch(pairs, sems):
    copies = [pltpu.make_async_copy(src, dst, sems.at[i]) for i, (src, dst) in enumerate(pairs)]
    for copy in copies:
        copy.start()
    return copies


def rim_kernel(half_ref, plane_ref, x_ref, b_ref, c_ref, out_ref, sems):
    start, pairs = 0, []
    for ref in (x_ref, b_ref, c_ref):
        rows, size = ref.shape
        pairs.append((ref.at[rows - 8 : rows, :], out_ref.at[:, start : start + size]))
        start += size
    for copy in fetch(pairs, sems):
        copy.wait()


def filtered(ext_ref, taps, lanes, first, count):
    total = taps[0:1] * ext_ref[first : first + count, lanes]
    for k in range(1, 4):
        total = total + taps[k : k + 1] * ext_ref[first + k : first + k + count, lanes]
    return silu(total)


def front_kernel(x_hbm, b_hbm, c_hbm, dt_hbm, pld_hbm, tx_hbm, tb_hbm, tc_hbm, bias_hbm, rate_hbm,
                 sig_ref, wv_ref, rv_ref, cum_ref, rows_ref, dtv_ref, s0_ref, s1_ref, begin_ref, taps_ref,
                 x_ref, b_ref, c_ref, dt_ref, pld_ref, tx_ref, tb_ref, tc_ref, bias_ref, rate_ref, ext_ref, wide_ref, sems):
    length, chans = x_ref.shape
    vecs = b_ref.shape[1]
    heads = dt_ref.shape[0]
    groups = vecs // STATE
    width = chans // groups
    copies = fetch((
        (bias_hbm, bias_ref), (rate_hbm, rate_ref), (dt_hbm, dt_ref), (pld_hbm, pld_ref), (tx_hbm, tx_ref), (tb_hbm, tb_ref),
        (tc_hbm, tc_ref), (b_hbm, b_ref), (c_hbm, c_ref), (x_hbm, x_ref),
    ), sems)
    for copy in copies[0:4]:
        copy.wait()
    wide_ref[...] = jnp.zeros_like(wide_ref)
    wide_ref[0:1, 0:heads] = bias_ref[...]
    wide_ref[1:2, 0:heads] = rate_ref[...]
    columns = wide_ref[:, 0:LANES].T
    v = dt_ref[...].astype(F32) + columns[0:heads, 0:1]
    step = jnp.maximum(v, 0.0) + jnp.log(1.0 + jnp.exp(-jnp.abs(v)))
    logs = pld_ref[...] - columns[0:heads, 1:2] * step
    upper = jnp.where(iota((length, length), 0) <= iota((length, length), 1), 1.0, 0.0)
    sums = mm(logs, upper, precision=lax.Precision.HIGHEST)
    rows_ref[...] = sums
    wide_ref[0:heads, :] = step
    dtv_ref[...] = wide_ref[...].T
    wide_ref[0:heads, :] = sums
    cum = wide_ref[...].T
    cum_ref[...] = cum
    half_end, end = cum[BLK - 1 : BLK], cum[length - 1 : length]
    ends = jnp.where(iota((length, LANES), 0) < BLK, half_end, end)
    weights = jnp.where(iota((length, LANES), 0) < HEAD, 0.0, dtv_ref[...] * jnp.exp(ends - cum))
    scale = spread(weights, head_lanes(chans))
    for copy in copies[4:7]:
        copy.wait()
    taps_ref[...] = jnp.zeros_like(taps_ref)
    sources = (
        (b_ref, tb_ref, chans, vecs, wv_ref, copies[7]), (c_ref, tc_ref, chans + vecs, vecs, rv_ref, copies[8]),
        (x_ref, tx_ref, 0, chans, sig_ref, copies[9]),
    )
    ext_ref[0:8, :] = jnp.zeros((8, ext_ref.shape[1]), F32)
    for src, taps, start, size, dst, copy in sources:
        taps_ref[0:4, start : start + size] = taps[...].astype(F32)
        copy.wait()
        ext_ref[8 : 8 + length, start : start + size] = src[...].astype(F32)
        begin_ref[:, start : start + size] = src[0:HEAD, :].astype(F32)
        for at in range(0, size, 256):
            lanes = slice(start + at, start + at + 256)
            dst[:, at : at + 256] = filtered(ext_ref, taps_ref[:, lanes], lanes, 5, length).astype(dst.dtype)
    for g in range(groups):
        part = slice(g * width, (g + 1) * width)
        vec = slice(g * STATE, (g + 1) * STATE)
        scaled = (sig_ref[:, part] * scale[:, part]).astype(BF16)
        s0_ref[:, part] = mm(wv_ref[0:BLK, vec], scaled[0:BLK], ((0,), (0,)))
        s1_ref[:, part] = mm(wv_ref[BLK:length, vec], scaled[BLK:length], ((0,), (0,)))


def head_kernel(rim_ref, begin_ref, taps_ref, siga_ref, wva_ref, rva_ref, cum_ref, dtv_ref, s0a_ref, s1_ref,
                sig_ref, wv_ref, rv_ref, s0_ref, send_ref, ext_ref):
    length, chans = siga_ref.shape
    vecs = wva_ref.shape[1]
    groups = vecs // STATE
    width = chans // groups
    ext_ref[0:8, :] = rim_ref[...].astype(F32)
    ext_ref[8 : 8 + HEAD, :] = begin_ref[...]
    for start, size, old, new in ((0, chans, siga_ref, sig_ref), (chans, vecs, wva_ref, wv_ref), (chans + vecs, vecs, rva_ref, rv_ref)):
        lanes = slice(start, start + size)
        new[0:HEAD, :] = filtered(ext_ref, taps_ref[:, lanes], lanes, 5, HEAD).astype(new.dtype)
        new[HEAD:, :] = old[HEAD:, :]
    half_end, end = cum_ref[BLK - 1 : BLK, :], cum_ref[length - 1 : length, :]
    lanes = head_lanes(chans)
    scale = spread(dtv_ref[0:HEAD, :] * jnp.exp(half_end - cum_ref[0:HEAD, :]), lanes)
    passing = spread(jnp.broadcast_to(jnp.exp(end - half_end), (8, LANES)), lanes)[0:1]
    scaled = (sig_ref[0:HEAD, :] * scale).astype(BF16)
    for g in range(groups):
        part = slice(g * width, (g + 1) * width)
        first = s0a_ref[:, part] + mm(wv_ref[0:HEAD, g * STATE : (g + 1) * STATE], scaled[:, part], ((0,), (0,)))
        s0_ref[:, part] = first
        send_ref[:, part] = (first * passing[:, part] + s1_ref[:, part]).astype(BF16)
    high = end.astype(BF16).astype(F32)
    mid = (end - high).astype(BF16).astype(F32)
    low = (end - high - mid).astype(BF16).astype(F32)
    row = iota((STATE, LANES), 0) % 8
    send_ref[:, chans : chans + LANES] = jnp.where(
        row == 0, high, jnp.where(row == 1, mid, jnp.where(row == 2, low, 0.0))
    ).astype(BF16)


def plane_kernel(got_ref, pin_ref, pdec_ref, send_ref):
    count = got_ref.shape[0] // 8
    chans = got_ref.shape[1] - LANES
    logs = jnp.sum(got_ref[:, chans:].astype(F32).reshape(count, 8, LANES), axis=1)
    lanes = head_lanes(chans)
    decay = spread(jnp.exp(logs), lanes)
    state = jnp.zeros((8, chans), F32)
    sofar = jnp.zeros((1, LANES), F32)
    before = []
    for i in range(count):
        pin_ref[8 * i : 8 * i + 8, :] = state
        before.append(sofar)
        state = state * decay[i : i + 1] + got_ref[8 * i : 8 * i + 8, 0:chans].astype(F32)
        sofar = sofar + logs[i : i + 1]
    pdec_ref[...] = spread(jnp.exp(jnp.concatenate(before, axis=0)), lanes)
    for k in range(send_ref.shape[0] // 8):
        send_ref[8 * k : 8 * k + 8, 0:chans] = state
        send_ref[8 * k : 8 * k + 8, chans:] = jnp.broadcast_to(sofar, (8, LANES))


def planes_kernel(plane_ref, pin_ref, pdec_ref, got_ref, out_ref):
    chans = pin_ref.shape[1]
    count = pin_ref.shape[0] // 8
    lanes = head_lanes(chans)
    plane = plane_ref[0]
    state = jnp.zeros((8, chans), F32)
    for k in range(got_ref.shape[0] // 8 - 1):
        rows = slice(8 * k, 8 * k + 8)
        state = jnp.where(k < plane, state * spread(jnp.exp(got_ref[rows, chans:]), lanes) + got_ref[rows, 0:chans], state)
    for i in range(0, count, 2):
        pair = [pin_ref[8 * k : 8 * k + 8, :] + state * pdec_ref[k : k + 1, :] for k in (i, i + 1)]
        out_ref[8 * i : 8 * i + 16, :] = jnp.concatenate(pair, axis=0).astype(BF16)


def near_kernel(sig_ref, wv_ref, rv_ref, cum_ref, rows_ref, dtv_ref, s0_ref, direct_ref, chosen_ref, y_ref, both_hbm, pad_ref, both_ref, sem):
    experts, tokens = both_ref.shape[0] // WIDE, chosen_ref.shape[1]
    slots = mm(expert_rows(experts), slot_table(chosen_ref[...], experts).astype(BF16))
    place = (iota(slots.shape, 0) % WIDE).astype(F32)
    both_ref[:, 0:tokens] = jnp.where(slots == place + 1.0, 1.0, 0.0).astype(BF16)
    for q in range(3):
        tail = jnp.where((place >= 6.0) & (slots == 3.0 * place + (q - 17.0)), 1.0, 0.0)
        both_ref[:, tokens * (q + 1) : tokens * (q + 2)] = tail.astype(BF16)
    copy = pltpu.make_async_copy(both_ref, both_hbm, sem)
    copy.start()
    length, chans = sig_ref.shape
    heads = direct_ref.shape[1]
    groups = wv_ref.shape[1] // STATE
    width = chans // groups
    lanes = head_lanes(chans)
    cum = cum_ref[...]
    cum_rows = rows_ref[...]
    pad_ref[...] = jnp.zeros_like(pad_ref)
    pad_ref[:, 0:heads] = jnp.broadcast_to(direct_ref[...], (8, heads))
    direct = spread(pad_ref[...], lanes)[0:1]
    scaled = (sig_ref[...] * spread(dtv_ref[...], lanes)).astype(BF16)
    causal = iota((BLK, BLK), 0) >= iota((BLK, BLK), 1)
    left = iota((BLK, LANES), 1) < HEAD_DIM
    into = spread(jnp.exp(cum[BLK:length] - cum[BLK - 1 : BLK]), lanes)
    for b in range(length // BLK):
        rows = slice(b * BLK, (b + 1) * BLK)
        for g in range(groups):
            vec = slice(g * STATE, (g + 1) * STATE)
            part = slice(g * width, (g + 1) * width)
            products = mm(rv_ref[rows, vec], wv_ref[rows, vec], ((1,), (1,)))
            if b == 1:
                carried = mm(rv_ref[rows, vec], s0_ref[:, part].astype(BF16)) * into[:, part]
            for j in range(width // LANES):
                at = g * width + j * LANES
                mats = []
                for h in (at // HEAD_DIM, at // HEAD_DIM + 1):
                    gap = cum[rows, h : h + 1] - cum_rows[h : h + 1, rows]
                    mats.append((products * jnp.exp(jnp.where(causal, gap, -1e30))).astype(BF16))
                pair = scaled[rows, at : at + LANES]
                zero = jnp.zeros_like(pair)
                stacked = jnp.concatenate([jnp.where(left, pair, zero), jnp.where(left, zero, pair)], axis=0)
                out = mm(jnp.concatenate(mats, axis=1), stacked)
                out = out + direct[:, at : at + LANES] * sig_ref[rows, at : at + LANES]
                if b == 1:
                    out = out + carried[:, j * LANES : (j + 1) * LANES]
                y_ref[rows, at : at + LANES] = out
    copy.wait()


def project_kernel(half_ref, y_ref, state_ref, rv_ref, cum_ref, gate_hbm, gain_hbm, w_hbm, other_ref, mine_ref, w_ref,
                   gate_ref, gain_ref, mix_ref, sems):
    length, chans = y_ref.shape
    groups = rv_ref.shape[1] // STATE
    width = chans // groups
    rows, dim = other_ref.shape
    parts = 4
    pairs = [(gate_hbm, gate_ref), (gain_hbm, gain_ref)]
    for k in range(parts):
        part = pl.ds(k * (dim // parts), dim // parts)
        pairs.append((w_hbm.at[:, part], w_ref.at[:, part]))
    copies = fetch(pairs, sems)
    scale = spread(jnp.exp(cum_ref[...]), head_lanes(chans))
    for g in range(groups):
        part = slice(g * width, (g + 1) * width)
        far = mm(rv_ref[:, g * STATE : (g + 1) * STATE], state_ref[:, part])
        inner = y_ref[:, part] + far * scale[:, part]
        if g == 0:
            copies[0].wait()
            copies[1].wait()
        gated = inner * silu(gate_ref[:, part].astype(F32))
        mean = jnp.sum(gated * gated, axis=1, keepdims=True) * (1.0 / width)
        mix_ref[:, part] = (gated * lax.rsqrt(mean + 1e-06) * gain_ref[:, part]).astype(BF16)
    half = half_ref[0]
    mine_ref[...] = mix_ref[pl.ds(pl.multiple_of(half * rows, rows), rows), :]
    theirs = mix_ref[pl.ds(pl.multiple_of((1 - half) * rows, rows), rows), :]
    for k in range(parts):
        part = slice(k * (dim // parts), (k + 1) * (dim // parts))
        copies[2 + k].wait()
        other_ref[:, part] = mm(theirs, w_ref[:, part]).astype(BF16)


def own_kernel(mine_ref, w_ref, stream_hbm, both_hbm, gain_hbm, own_ref, both_ref, gain_ref, stream_ref, sems):
    copies = fetch(((stream_hbm, stream_ref), (both_hbm, both_ref), (gain_hbm, gain_ref)), sems)
    product = mm(mine_ref[...], w_ref[...])
    copies[0].wait()
    own_ref[...] = product + stream_ref[...].astype(F32)
    for copy in copies[1:]:
        copy.wait()


def slot_table(chosen, experts):
    count = chosen.shape[1]
    expert = iota((experts, count), 0)
    named = jnp.zeros((experts, count), F32)
    for k in range(chosen.shape[0]):
        named = named + jnp.where(chosen[k : k + 1, :] == expert, 1.0, 0.0)
    earlier = jnp.where(iota((count, count), 0) < iota((count, count), 1), 1.0, 0.0).astype(BF16)
    return named * (mm(named.astype(BF16), earlier) + 1.0)


def expert_rows(experts):
    return jnp.where(iota((experts * WIDE, experts), 0) // WIDE == iota((experts * WIDE, experts), 1), 1.0, 0.0).astype(BF16)


def dispatch_kernel(own_ref, got_ref, both_ref, gain_ref, residual_ref, normed_ref, out_ref):
    rows, dim = own_ref.shape
    third = out_ref.shape[1] // 3
    residual = (own_ref[...] + got_ref[...].astype(F32)).astype(BF16)
    residual_ref[...] = residual
    wide = residual.astype(F32)
    mean = jnp.sum(wide * wide, axis=1, keepdims=True) * (1.0 / dim)
    normed_ref[...] = (wide * lax.rsqrt(mean + 1e-06) * gain_ref[...]).astype(BF16)
    main = both_ref[:, 0:rows]
    for q in range(3):
        mats = jnp.concatenate([main, both_ref[:, rows * (q + 1) : rows * (q + 2)]], axis=1)
        source = jnp.concatenate([normed_ref[:, q * third : (q + 1) * third], normed_ref[:, 3 * third :]], axis=0)
        out_ref[:, q * third : (q + 1) * third] = mm(mats, source).astype(BF16)


def shared_kernel(normed_ref, residual_ref, gate_ref, up_ref, down_ref, chosen_ref, weight_ref, out_ref, mats_ref):
    @pl.when(pl.program_id(0) == 0)
    def _():
        out_ref[...] = residual_ref[...].astype(F32)
        rows = normed_ref.shape[0]
        experts = mats_ref.shape[1] // WIDE
        chosen = chosen_ref[...]
        expert = iota((experts, rows), 0)
        weights = jnp.zeros((experts, rows), F32)
        for k in range(chosen.shape[0]):
            weights = weights + jnp.where(chosen[k : k + 1, :] == expert, weight_ref[k : k + 1, :], 0.0)
        lanes = expert_rows(experts)
        slots = mm(slot_table(chosen, experts).T.astype(BF16), lanes, ((1,), (1,)))
        spread_weights = mm(weights.T.astype(BF16), lanes, ((1,), (1,)))
        place = (iota(slots.shape, 1) % WIDE).astype(F32)
        mats_ref[0:rows, :] = jnp.where(slots == place + 1.0, spread_weights, 0.0).astype(BF16)
        for k in range(3):
            hit = (place >= 6.0) & (slots == 3.0 * place + (k - 17.0))
            mats_ref[rows * (k + 1) : rows * (k + 2), :] = jnp.where(hit, spread_weights, 0.0).astype(BF16)

    normed = normed_ref[...]
    hidden = (silu(mm(normed, gate_ref[...])) * mm(normed, up_ref[...])).astype(BF16)
    out_ref[...] += mm(hidden, down_ref[...])


def turn(value, by):
    return pltpu.roll(value, by % WIDE, axis=1)


def compact(value):
    width = value.shape[1]
    value = value.reshape(-1, 4, WIDE, width)
    row = iota((value.shape[0], WIDE, width), 1)
    a, b, c = turn(value[:, 1], 6), turn(value[:, 2], 4), turn(value[:, 3], 2)
    out = [jnp.where(row < 6, value[:, 0], a), jnp.where(row < 4, a, b), jnp.where(row < 2, b, c)]
    return jnp.concatenate(out, axis=1).reshape(-1, width)


def expand(value):
    value = value.reshape(-1, 3 * WIDE, value.shape[1])
    a, b, c = value[:, 0:WIDE], value[:, WIDE : 2 * WIDE], value[:, 2 * WIDE :]
    row = iota(a.shape, 1)
    return [a, jnp.where(row < 2, turn(a, 2), turn(b, 2)), jnp.where(row < 4, turn(b, 4), turn(c, 4)), turn(c, 6)]


def expert_kernel(x_ref, gate_ref, up_ref, down_ref, out_hbm, full_ref, out_ref, sems):
    total, wide = x_ref.shape
    third = wide // 3
    rows = out_ref.shape[1]
    row = iota((LANES // WIDE, WIDE, third), 1)
    copies = []
    for n in range(total // rows):
        for at in range(0, rows, LANES):
            dense = slice(at * SLOTS // WIDE, (at + LANES) * SLOTS // WIDE)
            tail = jnp.zeros(row.shape, F32)
            for q in range(3):
                part = x_ref[n * rows + at : n * rows + at + LANES, q * third : (q + 1) * third].astype(F32)
                full_ref[dense, q * third : (q + 1) * third] = compact(part).astype(BF16)
                part = part.reshape(row.shape)
                tail = jnp.where(row == q, turn(part, q - 6), jnp.where(row == 3 + q, turn(part, q - 4), tail))
            full_ref[dense, wide:] = compact(tail.reshape(LANES, third)).astype(BF16)
        full = full_ref[...]
        hidden = (silu(mm(full, gate_ref[...])) * mm(full, up_ref[...])).astype(BF16)
        tails = expand(mm(hidden, down_ref[:, wide:]))
        for q in range(3):
            part = slice(q * third, (q + 1) * third)
            mains = expand(mm(hidden, down_ref[:, part]))
            at = iota(mains[0].shape, 1)
            mixed = [
                jnp.where(at < 6, main, jnp.where(at == 6, turn(tail, 6 - q), turn(tail, 4 - q)))
                for main, tail in zip(mains, tails)
            ]
            out_ref[n, :, part] = jnp.stack(mixed, axis=1).reshape(rows, third).astype(BF16)
        copy = pltpu.make_async_copy(out_ref.at[n], out_hbm.at[n * rows : (n + 1) * rows, :], sems.at[n])
        copy.start()
        copies.append(copy)
    for copy in copies:
        copy.wait()


def combine_kernel(got_ref, base_hbm, mats_hbm, out_ref, base_ref, mats_ref, main_ref, sems):
    rows, dim = base_ref.shape
    third = got_ref.shape[1] // 3
    copies = fetch((
        (mats_hbm.at[0 : 2 * rows, :], mats_ref.at[0 : 2 * rows, :]), (mats_hbm.at[2 * rows :, :], mats_ref.at[2 * rows :, :]),
        (base_hbm, base_ref),
    ), sems)
    copies[0].wait()
    both = mm(mats_ref[0 : 2 * rows, :], got_ref[:, 0:third])
    main_ref[:, 0:third], tail = both[0:rows], both[rows:]
    copies[1].wait()
    for q in (1, 2):
        got = got_ref[:, q * third : (q + 1) * third]
        main_ref[:, q * third : (q + 1) * third] = mm(mats_ref[0:rows, :], got)
        tail = tail + mm(mats_ref[rows * (q + 1) : rows * (q + 2), :], got)
    copies[2].wait()
    out_ref[:, 0 : 3 * third] = (base_ref[:, 0 : 3 * third] + main_ref[...]).astype(BF16)
    out_ref[:, 3 * third :] = (base_ref[:, 3 * third :] + tail).astype(BF16)


def shape(dims, dtype=F32):
    return jax.ShapeDtypeStruct(dims, dtype)


def on_device(
    stream,
    head_input_signal,
    write_input_vectors,
    read_input_vectors,
    output_gate_input,
    step_size_input,
    position_log_decay,
    signal_filter_taps,
    write_filter_taps,
    read_filter_taps,
    step_size_bias,
    head_decay_rate,
    head_direct_term,
    grouped_norm_gain,
    mixer_output_weight,
    expert_norm_gain,
    chosen_expert_index,
    chosen_expert_weight,
    routed_gate_weight,
    routed_up_weight,
    routed_down_weight,
    common_gate_weight,
    common_up_weight,
    common_down_weight,
):
    length, chans = head_input_signal.shape
    vecs = write_input_vectors.shape[1]
    rows, dim = stream.shape
    hidden = common_gate_weight.shape[1]
    experts = lax.axis_size(SP_TP)
    wide = dim * SLOTS // WIDE

    heads = step_size_input.shape[1]
    devices = lax.axis_size(SP)
    half = lax.axis_index("tp").astype(jnp.int32).reshape(1)
    plane = lax.axis_index("sp_0").astype(jnp.int32).reshape(1)
    rim = pl.pallas_call(
        rim_kernel,
        in_specs=[pl.BlockSpec(memory_space=pltpu.SMEM)] * 2 + offchip(3),
        out_specs=onchip(1)[0],
        out_shape=shape((8, chans + 2 * vecs), BF16),
        scratch_shapes=[pltpu.SemaphoreType.DMA((3,))],
        compiler_params=room(2),
        name="rim",
    )(half, plane, *stay(head_input_signal, write_input_vectors, read_input_vectors))
    rim = lax.ppermute(rim, SP, [(i, i + 1) for i in range(devices - 1)])
    signal, write_rows, read_rows, cum, cum_rows, dtv, first, second, begin, taps = pl.pallas_call(
        front_kernel,
        in_specs=offchip(10),
        out_specs=tuple(onchip(10)),
        out_shape=(
            shape((length, chans)), shape((length, vecs), BF16), shape((length, vecs), BF16), shape((length, LANES)),
            shape((heads, length)), shape((length, LANES)), shape((STATE, chans)), shape((STATE, chans)),
            shape((HEAD, chans + 2 * vecs)), shape((8, chans + 2 * vecs)),
        ),
        scratch_shapes=[
            pltpu.VMEM((length, chans), BF16), pltpu.VMEM((length, vecs), BF16), pltpu.VMEM((length, vecs), BF16),
            pltpu.VMEM((heads, length), BF16), pltpu.VMEM((heads, length), F32),
            pltpu.VMEM((4, chans), BF16), pltpu.VMEM((4, vecs), BF16), pltpu.VMEM((4, vecs), BF16),
            pltpu.VMEM((1, heads), F32), pltpu.VMEM((1, heads), F32),
            pltpu.VMEM((length + 8, chans + 2 * vecs), F32), pltpu.VMEM((LANES, length), F32),
            pltpu.SemaphoreType.DMA((10,)),
        ],
        cost_estimate=pl.CostEstimate(flops=800_000_000, transcendentals=1_000_000, bytes_accessed=4_000_000),
        compiler_params=room(14),
        name="front",
    )(*stay(
        head_input_signal, write_input_vectors, read_input_vectors, step_size_input.T, position_log_decay.T,
        signal_filter_taps, write_filter_taps, read_filter_taps, step_size_bias[None], head_decay_rate[None],
    ))
    sig, wv, rv, s0, send = pl.pallas_call(
        head_kernel,
        in_specs=onchip(10),
        out_specs=tuple(onchip(5)),
        out_shape=(
            shape((length, chans)), shape((length, vecs), BF16), shape((length, vecs), BF16),
            shape((STATE, chans)), shape((STATE, chans + LANES), BF16),
        ),
        scratch_shapes=[pltpu.VMEM((HEAD + 8, chans + 2 * vecs), F32)],
        compiler_params=room(8),
        name="head",
    )(rim, begin, taps, signal, write_rows, read_rows, cum, dtv, first, second)
    in_plane = lax.axis_size(PLANE)
    got = lax.all_to_all(send, PLANE, split_axis=0, concat_axis=0, tiled=True)
    chosen = chosen_expert_index.T
    near, both = pl.pallas_call(
        near_kernel,
        in_specs=onchip(9),
        out_specs=(onchip(1)[0], offchip(1)[0]),
        out_shape=(shape((length, chans)), pltpu.HBM((experts * WIDE, 4 * rows), BF16)),
        scratch_shapes=[pltpu.VMEM((8, LANES), F32), pltpu.VMEM((experts * WIDE, 4 * rows), BF16), pltpu.SemaphoreType.DMA],
        cost_estimate=pl.CostEstimate(flops=400_000_000, transcendentals=1_000_000, bytes_accessed=4_000_000),
        compiler_params=room(18),
        name="near",
    )(sig, wv, rv, cum, cum_rows, dtv, s0, head_direct_term[None], chosen)
    planes = lax.axis_size("sp_0")
    pin, pdec, total = pl.pallas_call(
        plane_kernel,
        in_specs=onchip(1),
        out_specs=tuple(onchip(3)),
        out_shape=(shape((STATE, chans)), shape((in_plane, chans)), shape((8 * planes, chans + LANES))),
        compiler_params=room(6),
        name="plane",
    )(got)
    lower = lax.all_to_all(total, "sp_0", split_axis=0, concat_axis=0, tiled=True)
    back = pl.pallas_call(
        planes_kernel,
        in_specs=[pl.BlockSpec(memory_space=pltpu.SMEM)] + onchip(3),
        out_specs=onchip(1)[0],
        out_shape=shape((STATE, chans), BF16),
        compiler_params=room(6),
        name="planes",
    )(plane, pin, pdec, lower)
    incoming = lax.all_to_all(back, PLANE, split_axis=0, concat_axis=0, tiled=True)

    other, mine, projection = pl.pallas_call(
        project_kernel,
        in_specs=[pl.BlockSpec(memory_space=pltpu.SMEM)] + onchip(4) + offchip(3),
        out_specs=tuple(onchip(3)),
        out_shape=(shape((rows, dim), BF16), shape((rows, chans), BF16), shape((chans, dim), BF16)),
        scratch_shapes=[
            pltpu.VMEM((length, chans), BF16), pltpu.VMEM((1, chans), F32), pltpu.VMEM((length, chans), BF16),
            pltpu.SemaphoreType.DMA((6,)),
        ],
        compiler_params=room(16),
        name="project",
    )(half, near, incoming, rv, cum, *stay(output_gate_input, grouped_norm_gain[None], mixer_output_weight))
    partner = lax.ppermute(other, "tp", [(0, 1), (1, 0)])
    own, both, gain = pl.pallas_call(
        own_kernel,
        in_specs=onchip(2) + offchip(3),
        out_specs=tuple(onchip(3)),
        out_shape=(shape((rows, dim)), shape((experts * WIDE, 4 * rows), BF16), shape((1, dim))),
        scratch_shapes=[pltpu.VMEM((rows, dim), BF16), pltpu.SemaphoreType.DMA((3,))],
        cost_estimate=pl.CostEstimate(flops=600_000_000, transcendentals=0, bytes_accessed=6_000_000),
        compiler_params=room(10),
        name="own",
    )(mine, projection, *stay(stream, both, expert_norm_gain[None]))

    residual, normed, outgoing = pl.pallas_call(
        dispatch_kernel,
        in_specs=onchip(4),
        out_specs=tuple(onchip(3)),
        out_shape=(shape((rows, dim), BF16), shape((rows, dim), BF16), shape((experts * WIDE, wide), BF16)),
        compiler_params=room(12),
        name="dispatch",
    )(own, partner, both, gain)
    arrived = lax.all_to_all(outgoing, SP_TP, split_axis=0, concat_axis=0, tiled=True)

    part = 128
    fanout = chosen.shape[0]
    base, mats = pl.pallas_call(
        shared_kernel,
        grid=(hidden // part,),
        in_specs=[
            whole((rows, dim)), whole((rows, dim)), pl.BlockSpec((dim, part), lambda n: (0, n)),
            pl.BlockSpec((dim, part), lambda n: (0, n)), pl.BlockSpec((part, dim), lambda n: (n, 0)),
            whole((fanout, rows)), whole((fanout, rows)),
        ],
        out_specs=(whole((rows, dim)), whole((4 * rows, experts * WIDE))),
        out_shape=(pltpu.HBM((rows, dim), F32), pltpu.HBM((4 * rows, experts * WIDE), BF16)),
        cost_estimate=pl.CostEstimate(flops=800_000_000, transcendentals=70_000, bytes_accessed=8_000_000),
        compiler_params=room(16),
        name="shared",
    )(normed, residual, *stay(common_gate_weight, common_up_weight, common_down_weight), chosen, chosen_expert_weight.T)

    chunks = 2
    tall = experts * WIDE // chunks
    served = pl.pallas_call(
        expert_kernel,
        in_specs=onchip(4),
        out_specs=offchip(1)[0],
        out_shape=pltpu.HBM((experts * WIDE, wide), BF16),
        scratch_shapes=[pltpu.VMEM((tall * SLOTS // WIDE, dim), BF16), pltpu.VMEM((chunks, tall, wide), BF16), pltpu.SemaphoreType.DMA((chunks,))],
        compiler_params=room(24),
        name="experts",
    )(arrived, routed_gate_weight[0], routed_up_weight[0], routed_down_weight[0])
    returned = lax.all_to_all(served, SP_TP, split_axis=0, concat_axis=0, tiled=True)

    return pl.pallas_call(
        combine_kernel,
        in_specs=onchip(1) + offchip(2),
        out_specs=onchip(1)[0],
        out_shape=shape((rows, dim), BF16),
        scratch_shapes=[pltpu.VMEM((rows, dim), F32), pltpu.VMEM((4 * rows, experts * WIDE), BF16), pltpu.VMEM((rows, wide), F32), pltpu.SemaphoreType.DMA((3,))],
        compiler_params=room(16),
        name="combine",
    )(returned, *stay(base, mats))


def solution(mesh):
    split = Mesh(mesh.devices.reshape(4, 4, 4, mesh.shape["tp"]), ("sp_0", "sp_1", "sp_2", "tp"))
    return jax.shard_map(
        on_device,
        mesh=split,
        in_specs=(
            P(SP_TP, None),
            P(SP, "tp"),
            P(SP, "tp"),
            P(SP, "tp"),
            P(SP, "tp"),
            P(SP, "tp"),
            P(SP, "tp"),
            P(None, "tp"),
            P(None, "tp"),
            P(None, "tp"),
            P("tp"),
            P("tp"),
            P("tp"),
            P("tp"),
            P("tp", None),
            P(),
            P(SP_TP, None),
            P(SP_TP, None),
            P(SP_TP, None, None),
            P(SP_TP, None, None),
            P(SP_TP, None, None),
            P(),
            P(),
            P(),
        ),
        out_specs=P(SP_TP, None),
        check_vma=False,
    )
```
